32 devices in a mesh: gr: 2 (over y), sp: 4 (over z), tp: 4 (over x, core).
Axes of the slice: x: 2, y: 2, z: 4, core: 2. Of those that a mesh axis runs over, the one named last changes fastest.
Arguments:
- tokens: bfloat16 [4, 1024, 4096], P('gr', ('sp', 'tp')), parts along dimension 0, may hold values from -6 to 6
- norm_gain: bfloat16 [4096], replicated, may hold values from 0.099609375 to 1.8984375
- key_weight: bfloat16 [4096, 1024], P(None, 'tp'), may hold values from -0.09375 to 0.09375
- value_weight: bfloat16 [4096, 1024], P(None, 'tp'), may hold values from -0.09375 to 0.09375
- cum_gates: float32 [4, 1024, 16], P('gr', 'sp', 'tp'), parts along dimension 0, may hold values from -173 to 0, as said below
- new_query: bfloat16 [4, 1024], P('gr', 'tp'), parts along dimension 0, may hold values from -240 to 240
- new_key: bfloat16 [4, 1024], P('gr', 'tp'), parts along dimension 0, may hold values from -6 to 6
- new_value: bfloat16 [4, 1024], P('gr', 'tp'), parts along dimension 0, may hold values from -6 to 6
- new_gate: float32 [4, 16], P('gr', 'tp'), parts along dimension 0, may hold values from -5 to -1.5
Outputs:
- key_cache: bfloat16 [4, 1024, 1024], P('gr', 'sp', 'tp'), parts along dimension 0
- value_cache: bfloat16 [4, 1024, 1024], P('gr', 'sp', 'tp'), parts along dimension 0
- readout: bfloat16 [4, 1024], P('gr', 'tp'), parts along dimension 0
The draws below stay inside these ranges and needn't reach their ends.
There are 2 independent parts, one for each index of `gr`. The reference program is written for one: setup_inputs(seed, part) draws one part's arguments, and reference() takes and returns one part's arrays. A program takes and returns all parts, laid end to end along the dimension named above; an argument that names none is the same for every part. Nothing has to cross between parts.
Inputs may be any that keep to these rules, and one draw needn't show every extreme that they name: `cum_gates`: along positions, for each prompt and head, the values never rise.
All inputs are finite; a program needn't handle non-finite values.
Results may differ from the reference program's by a relative error of at most 0.005.
The reference program's roundings to bfloat16 on the way (of `normed`) count: a program that leaves them out, or rounds other values in their place, can miss the bound.
Values may be sent and summed in bfloat16 or wider, within the bound.
A program may use at most 64 MiB of HBM per device.

```python
import jax
import jax.numpy as jnp
from jax import lax

D = 4096
HEAD_COUNT = 16
HD = 64
PROMPTS_PER_GROUP = 2
KW = 1024
PROMPT_LENGTH = 1024


def draw_cum_gates(key, part):
    key_pieces = jax.random.split(jax.random.fold_in(key, 11), 7)
    decaying_heads = jax.random.uniform(key_pieces[0], (PROMPTS_PER_GROUP, 1, HEAD_COUNT)) < 0.5
    slow_rate = jax.random.uniform(key_pieces[1], (PROMPTS_PER_GROUP, 1, HEAD_COUNT), jnp.float32, 0.5, 1.5) / PROMPT_LENGTH
    fast_rate = 1.0 / jax.random.uniform(key_pieces[2], (PROMPTS_PER_GROUP, 1, HEAD_COUNT), jnp.float32, 30.0, 100.0)
    base_rate = jnp.where(decaying_heads, slow_rate, fast_rate)
    block_size = max(PROMPT_LENGTH // 32, 1)
    token_positions = jnp.arange(PROMPT_LENGTH)
    block_ids = jnp.minimum(token_positions // block_size, 31)
    log_factor = jax.random.uniform(key_pieces[3], (PROMPTS_PER_GROUP, 32, HEAD_COUNT), jnp.float32, -1.05, 1.05)
    block_factor = jnp.exp(log_factor)[:, block_ids, :]
    noise = jax.random.uniform(key_pieces[4], (PROMPTS_PER_GROUP, PROMPT_LENGTH, HEAD_COUNT), jnp.float32, 0.5, 1.5)
    per_step_decay = base_rate * block_factor * noise
    segment_position = jax.random.randint(key_pieces[5], (PROMPTS_PER_GROUP, 3, HEAD_COUNT), 0, PROMPT_LENGTH)
    segment_length = jax.random.uniform(key_pieces[6], (PROMPTS_PER_GROUP, 3, HEAD_COUNT), jnp.float32, 0.22, 0.69)
    match_count = (token_positions[None, :, None, None] == segment_position[:, None, :, :]).astype(jnp.float32)
    prompt_segments = jnp.sum(match_count * segment_length[:, None, :, :], axis=2)
    per_step_decay = per_step_decay + prompt_segments * decaying_heads.astype(jnp.float32)
    return -jnp.cumsum(per_step_decay, axis=1)


def draw_new_query(key, part):
    key_pieces = jax.random.split(jax.random.fold_in(key, 23), 1)
    normal_part = jax.random.normal(key_pieces[0], (PROMPTS_PER_GROUP, HEAD_COUNT, HD), jnp.float32)
    values_out = jnp.clip(normal_part * 2.0, -12.0, 12.0)
    return values_out.reshape(PROMPTS_PER_GROUP, KW).astype(jnp.bfloat16)


def levels(key, shape, shards, least, largest):
    level, own = 1.0, jax.random.fold_in(key, 6)
    for dim, shards_of in shards:
        draws = jnp.exp(jax.random.uniform(jax.random.fold_in(own, dim), (shards_of,), jnp.float32, least / len(shards), largest / len(shards)))
        level = level * jnp.repeat(draws, shape[dim] // shards_of).reshape([-1 if axis == dim else 1 for axis in range(len(shape))])
    return level


def bell_draw(rng, shape, scale, most, cuts=(), kind=jnp.bfloat16):
    factor_of = levels(rng, shape, cuts, -0.22, 0.18) if cuts else 1.0
    result = jax.random.normal(rng, shape, jnp.float32) * scale * factor_of
    return jnp.minimum(jnp.maximum(result, -most), most).astype(kind)


def setup_inputs(seed: int = 0, part: int = 0) -> dict:
    key_list = jax.random.split(jax.random.key(seed), 10)
    part_keys = jax.random.split(jax.random.fold_in(key_list[9], part), 10)
    return {
        "tokens": bell_draw(part_keys[0], (PROMPTS_PER_GROUP, PROMPT_LENGTH, D), 1.0, 6.0, ((1, 16),)),
        "norm_gain": jnp.clip(1.0 + 0.18 * jax.random.normal(key_list[1], (D,), jnp.float32), 0.099609375, 1.8984375).astype(jnp.bfloat16),
        "key_weight": bell_draw(key_list[2], (D, KW), D ** -0.5, 0.09375, ((1, 4),)),
        "value_weight": bell_draw(key_list[3], (D, KW), D ** -0.5, 0.09375, ((1, 4),)),
        "cum_gates": draw_cum_gates(jax.random.fold_in(jax.random.fold_in(key_list[9], part), 71), part),
        "new_query": draw_new_query(jax.random.fold_in(jax.random.fold_in(key_list[9], part), 71), part),
        "new_key": bell_draw(part_keys[6], (PROMPTS_PER_GROUP, KW), 1.0, 6.0, ((1, 4),)),
        "new_value": bell_draw(part_keys[7], (PROMPTS_PER_GROUP, KW), 1.0, 6.0, ((1, 4),)),
        "new_gate": jnp.clip(-5.0 + 3.5 * jax.random.uniform(part_keys[8], (PROMPTS_PER_GROUP, HEAD_COUNT), jnp.float32) ** levels(part_keys[8], (PROMPTS_PER_GROUP, HEAD_COUNT), ((1, 4),), -0.2, 0.2), -5.0, -1.5),
    }


epsilon = 1e-06

def reference(tokens, norm_gain, key_weight, value_weight, cum_gates, new_query, new_key, new_value, new_gate):
    as_float = tokens.astype(jnp.float32)
    normed = (as_float * lax.rsqrt(lax.optimization_barrier(jnp.mean(as_float * as_float, axis=-1, keepdims=True)) + epsilon) * norm_gain.astype(jnp.float32)).astype(jnp.bfloat16)
    flat_rows = normed.reshape(PROMPTS_PER_GROUP * PROMPT_LENGTH, D)
    key_cache = jnp.dot(flat_rows, key_weight, preferred_element_type=jnp.float32).astype(jnp.bfloat16).reshape(PROMPTS_PER_GROUP, PROMPT_LENGTH, KW)
    value_cache = jnp.dot(flat_rows, value_weight, preferred_element_type=jnp.float32).astype(jnp.bfloat16).reshape(PROMPTS_PER_GROUP, PROMPT_LENGTH, KW)
    score_scale = HD ** (-0.5)
    queries = new_query.reshape(PROMPTS_PER_GROUP, HEAD_COUNT, HD).astype(jnp.float32)
    key_heads = key_cache.reshape(PROMPTS_PER_GROUP, PROMPT_LENGTH, HEAD_COUNT, HD).astype(jnp.float32)
    value_heads = value_cache.reshape(PROMPTS_PER_GROUP, PROMPT_LENGTH, HEAD_COUNT, HD).astype(jnp.float32)
    fresh_key = new_key.reshape(PROMPTS_PER_GROUP, HEAD_COUNT, HD).astype(jnp.float32)
    fresh_value = new_value.reshape(PROMPTS_PER_GROUP, HEAD_COUNT, HD).astype(jnp.float32)
    scores = jnp.einsum('shd,slhd->shl', queries, key_heads, precision=lax.Precision.HIGHEST) * score_scale
    scores = scores + (new_gate + cum_gates[:, PROMPT_LENGTH - 1, :])[:, :, None] - jnp.transpose(cum_gates, (0, 2, 1))
    fresh_score = lax.optimization_barrier(jnp.sum(queries * fresh_key, axis=-1)) * score_scale
    maxima = jnp.maximum(lax.optimization_barrier(jnp.max(scores, axis=-1)), fresh_score)
    weights = jnp.exp(scores - maxima[:, :, None])
    fresh_weight = jnp.exp(fresh_score - maxima)
    totals = lax.optimization_barrier(jnp.sum(weights, axis=-1)) + fresh_weight
    weighted = jnp.einsum('shl,slhd->shd', weights, value_heads, precision=lax.Precision.HIGHEST)
    weighted = weighted + fresh_weight[:, :, None] * fresh_value
    readout = (weighted / totals[:, :, None]).reshape(PROMPTS_PER_GROUP, KW).astype(jnp.bfloat16)
    return (key_cache, value_cache, readout)
```

```python
import functools

import jax
import jax.numpy as jnp
from jax import lax
from jax.experimental import pallas as pl
from jax.experimental.pallas import tpu as pltpu
from jax.sharding import PartitionSpec as P

HD = 64
CORES = 2
RAW = 1

epsilon = 1e-06
masked_score = -1e30
MESH = pl.DeviceIdType.MESH


def kernel(
    dims,
    tok_hbm, gain_hbm, wk_hbm, wv_hbm, gates_hbm, q_hbm, nk_hbm, nv_hbm, ng_hbm,
    kbuf, vbuf, ro_ref,
    tok, raw, inv, nb, rx, acc, wbuf, ybuf, gain_v, gain_row, gates_v, q_v, nk_v, nv_v, ng_v,
    inv_tx, inv_rx, qblock, gate_rep, stats_tx, stats_rx,
    loc_sem, raw_sem, w_sem, small_sem, hop_sem, ready_sem,
    sx_sem, rx_sem, si_sem, ri_sem, sw_sem, rw_sem, sy_sem, ry_sem, sz_sem, rz_sem,
):
    S, L, R, T, Z = dims
    X = T // CORES
    f32, bf = jnp.float32, jnp.bfloat16
    rows_each, D = tok.shape
    NC, KC = nb.shape[0], nb.shape[2]
    blocks = rows_each // R
    C = kbuf.shape[2]
    H = C // HD
    BL = T * L
    tp = lax.axis_index("tp")
    z = lax.axis_index("sp")
    x, c = tp // CORES, tp % CORES
    partner = x * CORES + (CORES - 1 - c)

    def peer(d):
        return {"tp": ((x + d) % X) * CORES + c}

    def rows(j):
        return pl.ds(j * R, R)

    barrier = pltpu.get_barrier_semaphore()
    for d in range(1, X):
        pl.semaphore_signal(barrier, inc=1, device_id=peer(d), device_id_type=MESH)
    sides = (z > 0).astype(jnp.int32) + (z < Z - 1).astype(jnp.int32)

    def greet_sides(sem):
        @pl.when(z > 0)
        def _():
            pl.semaphore_signal(sem, inc=1, device_id={"sp": z - 1}, device_id_type=MESH)

        @pl.when(z < Z - 1)
        def _():
            pl.semaphore_signal(sem, inc=1, device_id={"sp": z + 1}, device_id_type=MESH)

    greet_sides(barrier)
    pl.semaphore_signal(barrier, inc=1, device_id={"tp": partner}, device_id_type=MESH)

    first = [pltpu.make_async_copy(tok_hbm.at[:, pl.ds(k * KC, KC)], raw.at[k], raw_sem.at[k]) for k in range(RAW)]
    loads = [pltpu.make_async_copy(tok_hbm.at[rows(j)], tok.at[rows(j)], loc_sem.at[j]) for j in range(blocks)]
    small = [
        pltpu.make_async_copy(src, dst, small_sem.at[i])
        for i, (src, dst) in enumerate(
            [(gain_hbm, gain_v), (gates_hbm, gates_v.at[0]), (q_hbm, q_v.at[0]), (nk_hbm, nk_v), (nv_hbm, nv_v), (ng_hbm, ng_v)]
        )
    ]
    for copy in first:
        copy.start()
    for copy in loads:
        copy.start()
    for copy in small:
        copy.start()
    w_copies = [
        pltpu.make_async_copy(src, wbuf.at[:, pl.ds(2 * i * C, C)], w_sem.at[i]) for i, src in enumerate((wk_hbm, wv_hbm))
    ]

    def to_partner(src, dst, i):
        return pltpu.make_async_remote_copy(
            src, dst, sw_sem.at[i], rw_sem.at[i], device_id={"tp": partner}, device_id_type=MESH
        )

    shares = [
        to_partner(wk_hbm, wbuf.at[:, pl.ds(C, C)], 0),
        to_partner(wv_hbm, wbuf.at[:, pl.ds(3 * C, C)], 1),
        to_partner(gates_hbm, gates_v.at[1], 2),
        to_partner(q_hbm, q_v.at[1], 3),
    ]

    def x_copy(d, k):
        src = raw.at[k] if isinstance(k, int) and k < RAW else nb.at[k]
        return pltpu.make_async_remote_copy(
            src, rx.at[d - 1, k], sx_sem.at[d - 1, k], rx_sem.at[d - 1, k], device_id=peer(d), device_id_type=MESH
        )

    def inv_copy(d):
        return pltpu.make_async_remote_copy(
            inv_tx, inv_rx.at[d - 1], si_sem.at[d - 1], ri_sem.at[d - 1], device_id=peer(d), device_id_type=MESH
        )

    def norm(v, r, k):
        return (v.astype(f32) * r * gain_row[:, pl.ds(k * KC, KC)]).astype(bf)

    for copy in first:
        copy.wait()
    pl.semaphore_wait(barrier, 1 + (X - 1) + sides)
    for k in range(RAW):
        for d in range(1, X):
            x_copy(d, k).start()

    small[0].wait()
    g = gain_v[...].astype(f32)
    lanes = g.shape[1]
    for i in range(g.shape[0]):
        gain_row[:, pl.ds(i * lanes, lanes)] = g[i : i + 1, :]
    for j in range(blocks):
        loads[j].wait()
        v = tok[rows(j), :].astype(f32)
        r = lax.rsqrt(jnp.mean(v * v, axis=-1, keepdims=True) + epsilon)
        inv[rows(j), :] = jnp.broadcast_to(r, (R, KC))
    for copy in w_copies:
        copy.start()
    eye = lax.broadcasted_iota(jnp.int32, (rows_each, rows_each), 0) == lax.broadcasted_iota(
        jnp.int32, (rows_each, rows_each), 1
    )
    inv_tx[...] = jnp.sum(jnp.where(eye, inv[:, :rows_each], 0.0), axis=0, keepdims=True)
    for k in range(RAW, NC):
        nb[k] = norm(tok[:, pl.ds(k * KC, KC)], inv[...], k)
        for d in range(1, X):
            x_copy(d, k).start()
        if k == RAW:
            for d in range(1, X):
                inv_copy(d).start()
    for copy in shares:
        copy.start()
    for k in range(RAW):
        nb[k] = norm(raw[k], inv[...], k)
    if Z > 2:
        greet_sides(hop_sem.at[0])

    for copy in small[1:]:
        copy.wait()
    for i in (2, 3):
        shares[i].wait_recv()

    scale = HD ** (-0.5)
    lane_head = lax.broadcasted_iota(jnp.int32, (C, C), 1) // HD
    same_head = lane_head == lax.broadcasted_iota(jnp.int32, (C, C), 0) // HD
    diagonal = lax.broadcasted_iota(jnp.int32, (C, C), 0) == lax.broadcasted_iota(jnp.int32, (C, C), 1)
    own_head = lax.broadcasted_iota(jnp.int32, (H, C), 1) // HD == lax.broadcasted_iota(jnp.int32, (H, C), 0)
    heads_eye = lax.broadcasted_iota(jnp.int32, (H, H), 0) == lax.broadcasted_iota(jnp.int32, (H, H), 1)
    last_block = z == Z - 1

    def as_row(column):
        return jnp.sum(jnp.where(own_head, column, 0.0), axis=0, keepdims=True)

    def source(d):
        return ((x + X - d) % X) * CORES + c

    for s in range(S):
        for g in range(CORES):
            column = jnp.sum(jnp.where(diagonal, q_v[g, s : s + 1, :].astype(f32), 0.0), axis=1, keepdims=True)
            qblock[s, g] = jnp.where(same_head, column, 0.0).astype(bf)
    head_of_lane = lax.broadcasted_iota(jnp.int32, (L, C), 1) // HD
    for d in range(X):
        pick = lax.broadcasted_iota(jnp.int32, (L, BL), 1) == lax.broadcasted_iota(
            jnp.int32, (L, BL), 0
        ) + source(d) * L
        for s in range(S):
            for g in range(CORES):
                spread = jnp.zeros((L, C), f32)
                for h in range(H):
                    column = jnp.sum(jnp.where(pick, gates_v[g, s, h : h + 1, :], 0.0), axis=1, keepdims=True)
                    spread = jnp.where(head_of_lane == h, column, spread)
                gate_rep[d, s, g] = spread
    for s in range(S):
        fresh = jnp.dot(nk_v[s : s + 1, :], qblock[s, 0], preferred_element_type=f32) * scale
        own_gate = jnp.sum(jnp.where(heads_eye, ng_v[s : s + 1, :], 0.0), axis=1, keepdims=True)
        fresh = jnp.where(last_block, fresh - as_row(gates_v[0, s, :, BL - 1 : BL] + own_gate), masked_score)
        weight = jnp.where(last_block, jnp.ones_like(fresh), 0.0)
        stats_tx[0, 0, s : s + 1, :] = fresh
        stats_tx[0, 1, s : s + 1, :] = weight
        stats_tx[0, 2, s : s + 1, :] = weight * nv_v[s : s + 1, :].astype(f32)
        stats_tx[1, 0, s : s + 1, :] = jnp.full((1, C), masked_score, f32)
        stats_tx[1, 1, s : s + 1, :] = jnp.zeros((1, C), f32)
        stats_tx[1, 2, s : s + 1, :] = jnp.zeros((1, C), f32)

    for d in range(1, X):
        inv_copy(d).wait_recv()
        r = jnp.sum(jnp.where(eye, inv_rx[d - 1], 0.0), axis=1, keepdims=True)
        for k in range(RAW):
            x_copy(d, k).wait_recv()
            rx[d - 1, k] = norm(rx[d - 1, k], r, k)

    def w_part(k):
        return wbuf[pl.ds(k * KC if isinstance(k, int) else pl.multiple_of(k * KC, KC), KC), :]

    def y_copy(d, s, v):
        at = pl.ds(pl.multiple_of(source(d) * L, L), L)
        return pltpu.make_async_remote_copy(
            ybuf.at[d, v, pl.ds(s * L, L)], (kbuf, vbuf)[v].at[s, at],
            sy_sem.at[d, s, v], ry_sem.at[d, s, v], device_id={"tp": partner}, device_id_type=MESH,
        )

    def y_arrival(d, s, v):
        at = pl.ds(pl.multiple_of(((x + X - d) % X * CORES + (CORES - 1 - c)) * L, L), L)
        return pltpu.make_async_remote_copy(
            ybuf.at[d, v, pl.ds(s * L, L)], (kbuf, vbuf)[v].at[s, at],
            sy_sem.at[d, s, v], ry_sem.at[d, s, v], device_id={"tp": partner}, device_id_type=MESH,
        )

    def finish(d, y, last):
        for s in range(S):
            at = pl.ds(s * L, L)
            for g in range(CORES):
                keys = y[s * L : (s + 1) * L, g * C : (g + 1) * C]
                values = y[s * L : (s + 1) * L, (2 + g) * C : (3 + g) * C].astype(f32)
                scores = jnp.dot(keys, qblock[s, g], preferred_element_type=f32) * scale - gate_rep[d, s, g]
                before = stats_tx[g, 0, s : s + 1, :]
                top = jnp.maximum(jnp.max(scores, axis=0, keepdims=True), before)
                weights = jnp.exp(scores - top)
                factor = jnp.exp(before - top)
                total = jnp.sum(weights, axis=0, keepdims=True) + factor * stats_tx[g, 1, s : s + 1, :]
                weighted = jnp.sum(weights * values, axis=0, keepdims=True) + factor * stats_tx[g, 2, s : s + 1, :]
                for i, row in enumerate((top, total, weighted)):
                    stats_tx[g, i, s : s + 1, :] = row
                    if last and g == 0:
                        stats_rx[z, 0, i, s : s + 1, :] = row

    def deliver(d, y):
        place = pl.ds(pl.multiple_of(source(d) * L, L), L)
        for s in range(S):
            part = y[s * L : (s + 1) * L]
            kbuf[s, place, :] = part[:, :C]
            vbuf[s, place, :] = part[:, 2 * C : 3 * C]
        ybuf[d, 0] = y[:, C : 2 * C]
        ybuf[d, 1] = y[:, 3 * C :]

    def send_partner(d):
        for s in range(S):
            for v in range(2):
                y_copy(d, s, v).start()

    for copy in w_copies:
        copy.wait()
    for i in (0, 1):
        shares[i].wait_recv()
    acc[...] = jnp.zeros_like(acc)

    def near(k, carry):
        acc[...] += jnp.dot(nb[k], w_part(k), preferred_element_type=f32)
        return carry

    lax.fori_loop(0, NC, near, 0)
    y = acc[...].astype(bf)
    deliver(0, y)
    finish(0, y, X == 1)
    send_partner(0)
    for r in range(1, Z - 2):
        pl.semaphore_wait(hop_sem.at[r - 1], sides)
        greet_sides(hop_sem.at[r])
    if Z > 2:
        pl.semaphore_wait(hop_sem.at[Z - 3], sides)
    pl.semaphore_signal(ready_sem, inc=1, device_id={"tp": partner}, device_id_type=MESH)
    pl.semaphore_wait(ready_sem, 1)

    for d in range(1, X):
        acc[...] = jnp.zeros_like(acc)

        def far(k, carry, d=d):
            @pl.when(k >= RAW)
            def _():
                x_copy(d, k).wait_recv()

            acc[...] += jnp.dot(rx[d - 1, k], w_part(k), preferred_element_type=f32)
            return carry

        lax.fori_loop(0, NC - 1, far, 0)
        x_copy(d, NC - 1).wait_recv()
        y = (acc[...] + jnp.dot(rx[d - 1, NC - 1], w_part(NC - 1), preferred_element_type=f32)).astype(bf)
        if d < X - 1:
            deliver(d, y)
            finish(d, y, False)
            send_partner(d)
        else:
            finish(d, y, True)

    def z_copy(d, other):
        return pltpu.make_async_remote_copy(
            stats_tx.at[other], stats_rx.at[z, other], sz_sem.at[other, d], rz_sem.at[other, d],
            device_id={"sp": (z + d) % Z, "tp": partner if other else tp}, device_id_type=MESH,
        )

    sends = [(d, other) for other in range(CORES) for d in range(Z) if d or other]
    for d, other in sorted(sends, key=lambda e: -min(e[0], Z - e[0])):
        z_copy(d, other).start()
    if X > 1:
        deliver(X - 1, y)
        send_partner(X - 1)
    for d in range(1, X):
        inv_copy(d).wait_send()
        for k in range(NC):
            x_copy(d, k).wait_send()
    for copy in shares:
        copy.wait_send()
    for d in range(X):
        for s in range(S):
            for v in range(2):
                y_copy(d, s, v).wait_send()
                y_arrival(d, s, v).wait_recv()
    for d, other in sends:
        at = (z + Z - d) % Z
        pltpu.make_async_remote_copy(
            stats_tx.at[other], stats_rx.at[at, other], sz_sem.at[other, d], rz_sem.at[other, d],
            device_id={"sp": at, "tp": partner if other else tp}, device_id_type=MESH,
        ).wait_recv()
    everything = stats_rx[...].reshape(Z * CORES, 3, S, C)
    tops, totals, sums = everything[:, 0], everything[:, 1], everything[:, 2]
    factor = jnp.exp(tops - jnp.max(tops, axis=0, keepdims=True))
    ro_ref[...] = (jnp.sum(sums * factor, axis=0) / jnp.sum(totals * factor, axis=0)).astype(ro_ref.dtype)
    for d, other in sends:
        z_copy(d, other).wait_send()


def write_out(*refs):
    sems = refs[-1]
    count = (len(refs) - 1) // 2
    copies = [pltpu.make_async_copy(refs[i], refs[count + i], sems.at[i]) for i in range(count)]
    for copy in copies:
        copy.start()
    for copy in copies:
        copy.wait()


def body(
    tokens, norm_gain, key_weight, value_weight, cum_gates, new_query, new_key, new_value, new_gate
):
    S, L, D = tokens.shape
    C = key_weight.shape[1]
    H = C // HD
    T = lax.axis_size("tp")
    Z = lax.axis_size("sp")
    X = T // CORES
    BL = T * L
    R = 16 if L % 16 == 0 else L
    KC = 256 if D % 256 == 0 else D // 2
    NC = D // KC
    bf, f32 = jnp.bfloat16, jnp.float32
    hbm = pl.BlockSpec(memory_space=pltpu.HBM)
    dma = pltpu.SemaphoreType.DMA
    regular = pltpu.SemaphoreType.REGULAR
    far = max(X - 1, 1)
    vmem = pl.BlockSpec(memory_space=pltpu.VMEM)
    results = pl.pallas_call(
        functools.partial(kernel, (S, L, R, T, Z)),
        out_shape=(
            pltpu.VMEM((S, BL, C), bf),
            pltpu.VMEM((S, BL, C), bf),
            pltpu.VMEM((S, C), bf),
        ),
        in_specs=[hbm] * 9,
        out_specs=(vmem, vmem, vmem),
        scratch_shapes=[
            pltpu.VMEM((S * L, D), bf),
            pltpu.VMEM((RAW, S * L, KC), bf),
            pltpu.VMEM((S * L, KC), f32),
            pltpu.VMEM((NC, S * L, KC), bf),
            pltpu.VMEM((far, NC, S * L, KC), bf),
            pltpu.VMEM((S * L, 4 * C), f32),
            pltpu.VMEM((D, 4 * C), bf),
            pltpu.VMEM((X, 2, S * L, C), bf),
            pltpu.VMEM((D // 128, 128), bf),
            pltpu.VMEM((1, D), f32),
            pltpu.VMEM((CORES, S, H, BL), f32),
            pltpu.VMEM((CORES, S, C), bf),
            pltpu.VMEM((S, C), bf),
            pltpu.VMEM((S, C), bf),
            pltpu.VMEM((S, H), f32),
            pltpu.VMEM((1, S * L), f32),
            pltpu.VMEM((far, 1, S * L), f32),
            pltpu.VMEM((S, CORES, C, C), bf),
            pltpu.VMEM((X, S, CORES, L, C), f32),
            pltpu.VMEM((CORES, 3, S, C), f32),
            pltpu.VMEM((Z, CORES, 3, S, C), f32),
            dma((S * L // R,)), dma((RAW,)), dma((2,)), dma((6,)), regular((max(Z - 2, 1),)), regular,
            dma((far, NC)), dma((far, NC)), dma((far,)), dma((far,)), dma((4,)), dma((4,)),
            dma((X, S, 2)), dma((X, S, 2)), dma((CORES, Z)), dma((CORES, Z)),
        ],
        compiler_params=pltpu.CompilerParams(
            collective_id=0, has_side_effects=True, vmem_limit_bytes=56 * 1024 * 1024
        ),
    )(
        tokens.reshape(S * L, D),
        norm_gain.reshape(D // 128, 128),
        key_weight,
        value_weight,
        jnp.transpose(cum_gates, (0, 2, 1)),
        new_query,
        new_key,
        new_value,
        new_gate,
    )
    return pl.pallas_call(
        write_out,
        out_shape=tuple(jax.ShapeDtypeStruct(r.shape, r.dtype) for r in results),
        in_specs=[vmem] * 3,
        out_specs=(hbm, hbm, hbm),
        scratch_shapes=[dma((3,))],
    )(*(pltpu.with_memory_space_constraint(r, pltpu.VMEM) for r in results))


def solution(mesh):
    in_specs = (
        P("gr", ("sp", "tp"), None),
        P(),
        P(None, "tp"),
        P(None, "tp"),
        P("gr", "sp", "tp"),
        P("gr", "tp"),
        P("gr", "tp"),
        P("gr", "tp"),
        P("gr", "tp"),
    )
    out_specs = (P("gr", "sp", "tp"), P("gr", "sp", "tp"), P("gr", "tp"))
    return jax.shard_map(body, mesh=mesh, in_specs=in_specs, out_specs=out_specs, check_vma=False)
```

```python
import functools

import jax
import jax.numpy as jnp
from jax import lax
from jax.experimental import pallas as pl
from jax.experimental.pallas import tpu as pltpu
from jax.sharding import PartitionSpec as P

HD = 64
CORES = 2
LEAD = 4
RAW = 2

epsilon = 1e-06
masked_score = -1e30
MESH = pl.DeviceIdType.MESH


def kernel(
    dims,
    tok_hbm, gain_hbm, wk_hbm, wv_hbm, gates_hbm, q_hbm, nk_hbm, nv_hbm, ng_hbm,
    kbuf, vbuf, ro_ref,
    tok, raw, inv, nb, rx, acc, wbuf, ybuf, gain_v, gain_row, gates_v, new_v, ng_v,
    inv_tx, inv_rx, qblock, gate_rep, stats_tx, stats_rx,
    loc_sem, raw_sem, w_sem, small_sem, hop_sem, ready_sem,
    sx_sem, rx_sem, si_sem, ri_sem, sw_sem, rw_sem, sy_sem, ry_sem, sz_sem, rz_sem,
):
    S, L, R, T, Z = dims
    X = T // CORES
    f32, bf = jnp.float32, jnp.bfloat16
    rows_each, D = tok.shape
    NC, KC = nb.shape[0], nb.shape[2]
    blocks = rows_each // R
    C = kbuf.shape[2]
    H = C // HD
    BL = T * L
    tp = lax.axis_index("tp")
    z = lax.axis_index("sp")
    x, c = tp // CORES, tp % CORES
    partner = x * CORES + (CORES - 1 - c)

    def peer(d):
        return {"tp": ((x + d) % X) * CORES + c}

    def rows(j):
        return pl.ds(j * R, R)

    first = [pltpu.make_async_copy(tok_hbm.at[:, pl.ds(k * KC, KC)], raw.at[k], raw_sem) for k in range(RAW)]
    for copy in first:
        copy.start()
    barrier = pltpu.get_barrier_semaphore()
    for d in range(1, X):
        pl.semaphore_signal(barrier, inc=1, device_id=peer(d), device_id_type=MESH)
    sides = (z > 0).astype(jnp.int32) + (z < Z - 1).astype(jnp.int32)

    def greet_sides(sem):
        @pl.when(z > 0)
        def _():
            pl.semaphore_signal(sem, inc=1, device_id={"sp": z - 1}, device_id_type=MESH)

        @pl.when(z < Z - 1)
        def _():
            pl.semaphore_signal(sem, inc=1, device_id={"sp": z + 1}, device_id_type=MESH)

    greet_sides(barrier)
    pl.semaphore_signal(barrier, inc=1, device_id={"tp": partner}, device_id_type=MESH)

    loads = [pltpu.make_async_copy(tok_hbm.at[rows(j)], tok.at[rows(j)], loc_sem.at[j]) for j in range(blocks)]
    small = [
        pltpu.make_async_copy(src, dst, small_sem.at[min(i, 3)])
        for i, (src, dst) in enumerate(
            [(gain_hbm, gain_v), (gates_hbm, gates_v.at[0]), (ng_hbm, ng_v), (q_hbm, new_v.at[0]), (nk_hbm, new_v.at[1]), (nv_hbm, new_v.at[2])]
        )
    ]
    for copy in loads:
        copy.start()
    for copy in small:
        copy.start()
    w_copies = [
        pltpu.make_async_copy(src, wbuf.at[:, pl.ds(2 * i * C, C)], w_sem) for i, src in enumerate((wk_hbm, wv_hbm))
    ]

    def to_partner(src, dst, i):
        return pltpu.make_async_remote_copy(
            src, dst, sw_sem.at[i], rw_sem.at[i], device_id={"tp": partner}, device_id_type=MESH
        )

    shares = [
        to_partner(wk_hbm, wbuf.at[:, pl.ds(C, C)], 0),
        to_partner(wv_hbm, wbuf.at[:, pl.ds(3 * C, C)], 0),
        to_partner(gates_hbm, gates_v.at[1], 1),
        to_partner(q_hbm, new_v.at[3], 2),
    ]
    both_weights = to_partner(wbuf.at[:, pl.ds(0, 2 * C)], wbuf.at[:, pl.ds(0, 2 * C)], 0)

    groups = [(0, RAW)] + [g for g in ((RAW, NC // 2), (NC // 2, NC - 2), (NC - 2, NC - 1)) if g[0] < g[1]] + [(NC - 1, NC)]

    def group_of(k):
        return next(i for i, (a, b) in enumerate(groups) if a <= k < b)

    def x_copy(d, k):
        src = raw.at[k] if k < RAW else nb.at[k]
        return pltpu.make_async_remote_copy(
            src, rx.at[d - 1, k], sx_sem.at[d - 1], rx_sem.at[d - 1, group_of(k)], device_id=peer(d), device_id_type=MESH
        )

    def x_whole(d, first, count, group):
        part = rx.at[d - 1, pl.ds(first, count)]
        return pltpu.make_async_remote_copy(
            part, part, sx_sem.at[d - 1], rx_sem.at[d - 1, group], device_id=peer(d), device_id_type=MESH
        )

    def inv_copy(d):
        return pltpu.make_async_remote_copy(
            inv_tx, inv_rx.at[d - 1], si_sem.at[d - 1], ri_sem.at[d - 1], device_id=peer(d), device_id_type=MESH
        )

    def norm(v, r, k):
        return (v.astype(f32) * r * gain_row[:, pl.ds(k * KC, KC)]).astype(bf)

    pltpu.make_async_copy(raw, raw, raw_sem).wait()
    pl.semaphore_wait(barrier, 1 + (X - 1) + sides)

    def send(chunks):
        for k in chunks:
            for d in range(1, X):
                x_copy(d, k).start()

    pl.when(c == 0)(lambda: send(range(RAW)))
    pl.when(c != 0)(lambda: send(range(RAW)))

    small[0].wait()
    g = gain_v[...].astype(f32)
    lanes = g.shape[1]
    for i in range(g.shape[0]):
        gain_row[:, pl.ds(i * lanes, lanes)] = g[i : i + 1, :]
    for j in range(blocks):
        loads[j].wait()
        v = tok[rows(j), :].astype(f32)
        r = lax.rsqrt(jnp.mean(v * v, axis=-1, keepdims=True) + epsilon)
        inv[rows(j), :] = jnp.broadcast_to(r, (R, KC))
    for copy in w_copies:
        copy.start()
    eye = lax.broadcasted_iota(jnp.int32, (rows_each, rows_each), 0) == lax.broadcasted_iota(
        jnp.int32, (rows_each, rows_each), 1
    )
    inv_tx[...] = jnp.sum(jnp.where(eye, inv[:, :rows_each], 0.0), axis=0, keepdims=True)
    for k in range(RAW, NC):
        nb[k] = norm(tok[:, pl.ds(k * KC, KC)], inv[...], k)
        if k < LEAD:
            send([k])
        else:
            pl.when(c == 0)(lambda k=k: send([k]))
        if k == RAW:
            for d in range(1, X):
                inv_copy(d).start()
    for copy in shares[2:] + shares[:2]:
        copy.start()
    for k in range(RAW):
        nb[k] = norm(raw[k], inv[...], k)
    if Z > 2:
        greet_sides(hop_sem.at[0])

    @pl.when(c != 0)
    def _():
        for d in range(1, X):
            x_whole(d, 0, LEAD, 0).wait_send()

    small[1].wait()
    small[2].wait()
    pltpu.make_async_copy(new_v.at[pl.ds(0, 3)], new_v.at[pl.ds(0, 3)], small_sem.at[3]).wait()
    for i in (2, 3):
        shares[i].wait_recv()

    scale = HD ** (-0.5)
    lane_head = lax.broadcasted_iota(jnp.int32, (C, C), 1) // HD
    same_head = lane_head == lax.broadcasted_iota(jnp.int32, (C, C), 0) // HD
    diagonal = lax.broadcasted_iota(jnp.int32, (C, C), 0) == lax.broadcasted_iota(jnp.int32, (C, C), 1)
    own_head = lax.broadcasted_iota(jnp.int32, (H, C), 1) // HD == lax.broadcasted_iota(jnp.int32, (H, C), 0)
    heads_eye = lax.broadcasted_iota(jnp.int32, (H, H), 0) == lax.broadcasted_iota(jnp.int32, (H, H), 1)
    last_block = z == Z - 1

    def as_row(column):
        return jnp.sum(jnp.where(own_head, column, 0.0), axis=0, keepdims=True)

    def source(d):
        return ((x + X - d) % X) * CORES + c

    for s in range(S):
        for g in range(CORES):
            column = jnp.sum(jnp.where(diagonal, new_v[3 * g, s : s + 1, :].astype(f32), 0.0), axis=1, keepdims=True)
            qblock[s, g] = jnp.where(same_head, column, 0.0).astype(bf)
    head_of_lane = lax.broadcasted_iota(jnp.int32, (L, C), 1) // HD
    for d in range(X):
        pick = lax.broadcasted_iota(jnp.int32, (L, BL), 1) == lax.broadcasted_iota(
            jnp.int32, (L, BL), 0
        ) + source(d) * L
        for s in range(S):
            for g in range(CORES):
                spread = jnp.zeros((L, C), f32)
                for h in range(H):
                    column = jnp.sum(jnp.where(pick, gates_v[g, s, h : h + 1, :], 0.0), axis=1, keepdims=True)
                    spread = jnp.where(head_of_lane == h, column, spread)
                gate_rep[d, s, g] = spread
    for s in range(S):
        fresh = jnp.dot(new_v[1, s : s + 1, :], qblock[s, 0], preferred_element_type=f32) * scale
        own_gate = jnp.sum(jnp.where(heads_eye, ng_v[s : s + 1, :], 0.0), axis=1, keepdims=True)
        fresh = jnp.where(last_block, fresh - as_row(gates_v[0, s, :, BL - 1 : BL] + own_gate), masked_score)
        weight = jnp.where(last_block, jnp.ones_like(fresh), 0.0)
        stats_tx[0, 0, s : s + 1, :] = fresh
        stats_tx[0, 1, s : s + 1, :] = weight
        stats_tx[0, 2, s : s + 1, :] = weight * new_v[2, s : s + 1, :].astype(f32)
        stats_tx[1, 0, s : s + 1, :] = jnp.full((1, C), masked_score, f32)
        stats_tx[1, 1, s : s + 1, :] = jnp.zeros((1, C), f32)
        stats_tx[1, 2, s : s + 1, :] = jnp.zeros((1, C), f32)

    pl.when(c != 0)(lambda: send(range(LEAD, NC)))
    for d in range(1, X):
        inv_copy(d).wait_recv()
        r = jnp.sum(jnp.where(eye, inv_rx[d - 1], 0.0), axis=1, keepdims=True)
        x_whole(d, 0, RAW, 0).wait_recv()
        for k in range(RAW):
            rx[d - 1, k] = norm(rx[d - 1, k], r, k)

    def w_part(k):
        return wbuf[pl.ds(k * KC if isinstance(k, int) else pl.multiple_of(k * KC, KC), KC), :]

    def y_copy(d, s, v):
        at = pl.ds(pl.multiple_of(source(d) * L, L), L)
        return pltpu.make_async_remote_copy(
            ybuf.at[d, v, pl.ds(s * L, L)], (kbuf, vbuf)[v].at[s, at],
            sy_sem, ry_sem, device_id={"tp": partner}, device_id_type=MESH,
        )

    def finish(d, y, last):
        pairs = [(g, s) for g in range(CORES) for s in range(S)]
        before = {(g, s): [stats_tx[g, i, s : s + 1, :] for i in range(3)] for g, s in pairs}
        scores = {}
        for g, s in pairs:
            keys = y[s * L : (s + 1) * L, g * C : (g + 1) * C]
            scores[g, s] = jnp.dot(keys, qblock[s, g], preferred_element_type=f32) * scale - gate_rep[d, s, g]
        after = {}
        for g, s in pairs:
            old_top, old_total, old_weighted = before[g, s]
            values = y[s * L : (s + 1) * L, (2 + g) * C : (3 + g) * C].astype(f32)
            top = jnp.maximum(jnp.max(scores[g, s], axis=0, keepdims=True), old_top)
            weights = jnp.exp(scores[g, s] - top)
            factor = jnp.exp(old_top - top)
            total = jnp.sum(weights, axis=0, keepdims=True) + factor * old_total
            weighted = jnp.sum(weights * values, axis=0, keepdims=True) + factor * old_weighted
            after[g, s] = (top, total, weighted)
        for g, s in pairs:
            for i, row in enumerate(after[g, s]):
                stats_tx[g, i, s : s + 1, :] = row
        if last:
            for s in range(S):
                for i, row in enumerate(after[0, s]):
                    stats_rx[0, z, i, s : s + 1, :] = row

    def deliver(d, y):
        place = pl.ds(pl.multiple_of(source(d) * L, L), L)
        for s in range(S):
            part = y[s * L : (s + 1) * L]
            kbuf[s, place, :] = part[:, :C]
            vbuf[s, place, :] = part[:, 2 * C : 3 * C]
        ybuf[d, 0] = y[:, C : 2 * C]
        ybuf[d, 1] = y[:, 3 * C :]

    def send_partner(d):
        for s in range(S):
            for v in range(2):
                y_copy(d, s, v).start()

    pltpu.make_async_copy(wbuf.at[:, pl.ds(0, 2 * C)], wbuf.at[:, pl.ds(0, 2 * C)], w_sem).wait()
    both_weights.wait_recv()
    acc[...] = jnp.zeros_like(acc)

    def near(k, carry):
        acc[...] += jnp.dot(nb[k], w_part(k), preferred_element_type=f32)
        return carry

    lax.fori_loop(0, NC, near, 0)
    y = acc[...].astype(bf)
    deliver(0, y)
    finish(0, y, X == 1)
    send_partner(0)
    for r in range(1, Z - 2):
        pl.semaphore_wait(hop_sem.at[r - 1], sides)
        greet_sides(hop_sem.at[r])
    if Z > 2:
        pl.semaphore_wait(hop_sem.at[Z - 3], sides)
    pl.semaphore_signal(ready_sem, inc=1, device_id={"tp": partner}, device_id_type=MESH)
    pl.semaphore_wait(ready_sem, 1)

    for d in range(1, X):
        acc[...] = jnp.zeros_like(acc)

        def far(k, carry, d=d):
            acc[...] += jnp.dot(rx[d - 1, k], w_part(k), preferred_element_type=f32)
            return carry

        for i, (start, stop) in enumerate(groups[:-1]):
            if i:
                x_whole(d, start, stop - start, i).wait_recv()
            lax.fori_loop(start, stop, far, 0)
        x_whole(d, NC - 1, 1, len(groups) - 1).wait_recv()
        y = (acc[...] + jnp.dot(rx[d - 1, NC - 1], w_part(NC - 1), preferred_element_type=f32)).astype(bf)
        if d < X - 1:
            deliver(d, y)
            finish(d, y, False)
            send_partner(d)
        else:
            finish(d, y, True)

    def z_target(i):
        return jnp.where(2 * z >= Z, i, Z - 1 - i)

    def z_copy(i, other):
        to = z_target(i)
        return pltpu.make_async_remote_copy(
            stats_tx.at[other], stats_rx.at[other, z], sz_sem.at[other], rz_sem.at[other],
            device_id={"sp": to, "tp": partner if other else tp}, device_id_type=MESH,
        )

    for i in range(Z):
        for first_core in range(CORES):

            @pl.when(c == first_core)
            def _(i=i, first_core=first_core):
                for core in range(CORES):
                    if core == first_core:
                        pl.when(z_target(i) != z)(z_copy(i, 0).start)
                    else:
                        z_copy(i, 1).start()

    if X > 1:
        deliver(X - 1, y)
        send_partner(X - 1)
    for d in range(1, X):
        inv_copy(d).wait_send()
        pl.when(c == 0)(x_whole(d, 0, NC, 0).wait_send)
        pl.when(c != 0)(x_whole(d, LEAD, NC - LEAD, 0).wait_send)
    both_weights.wait_send()
    shares[2].wait_send()
    shares[3].wait_send()
    halves = pltpu.make_async_remote_copy(ybuf, ybuf, sy_sem, ry_sem, device_id={"tp": partner}, device_id_type=MESH)
    halves.wait_send()
    halves.wait_recv()

    def z_whole(other):
        part = stats_rx.at[other, pl.ds(0, Z - 1 + other)]
        return pltpu.make_async_remote_copy(
            part, part, sz_sem.at[other], rz_sem.at[other],
            device_id={"tp": partner if other else tp}, device_id_type=MESH,
        )

    for other in range(CORES):
        if Z - 1 + other:
            z_whole(other).wait_recv()
    entries = [(i, other) for i in range(Z) for other in range(CORES)]
    tops = [stats_rx[other, i, 0] for i, other in entries]
    most = functools.reduce(jnp.maximum, tops)
    factors = [jnp.exp(top - most) for top in tops]
    total = functools.reduce(jnp.add, [f * stats_rx[other, i, 1] for f, (i, other) in zip(factors, entries)])
    weighted = functools.reduce(jnp.add, [f * stats_rx[other, i, 2] for f, (i, other) in zip(factors, entries)])
    ro_ref[...] = (weighted / total).astype(ro_ref.dtype)
    for other in range(CORES):
        if Z - 1 + other:
            z_whole(other).wait_send()


def write_out(*refs):
    sems = refs[-1]
    count = (len(refs) - 1) // 2
    copies = [pltpu.make_async_copy(refs[i], refs[count + i], sems.at[i]) for i in range(count)]
    for copy in copies:
        copy.start()
    for copy in copies:
        copy.wait()


def body(
    tokens, norm_gain, key_weight, value_weight, cum_gates, new_query, new_key, new_value, new_gate
):
    S, L, D = tokens.shape
    C = key_weight.shape[1]
    H = C // HD
    T = lax.axis_size("tp")
    Z = lax.axis_size("sp")
    X = T // CORES
    BL = T * L
    R = 32 if L % 32 == 0 else L
    KC = 256 if D % 256 == 0 else D // 2
    NC = D // KC
    bf, f32 = jnp.bfloat16, jnp.float32
    hbm = pl.BlockSpec(memory_space=pltpu.HBM)
    dma = pltpu.SemaphoreType.DMA
    regular = pltpu.SemaphoreType.REGULAR
    far = max(X - 1, 1)
    vmem = pl.BlockSpec(memory_space=pltpu.VMEM)
    results = pl.pallas_call(
        functools.partial(kernel, (S, L, R, T, Z)),
        out_shape=(
            pltpu.VMEM((S, BL, C), bf),
            pltpu.VMEM((S, BL, C), bf),
            pltpu.VMEM((S, C), bf),
        ),
        in_specs=[hbm] * 9,
        out_specs=(vmem, vmem, vmem),
        scratch_shapes=[
            pltpu.VMEM((S * L, D), bf),
            pltpu.VMEM((RAW, S * L, KC), bf),
            pltpu.VMEM((S * L, KC), f32),
            pltpu.VMEM((NC, S * L, KC), bf),
            pltpu.VMEM((far, NC, S * L, KC), bf),
            pltpu.VMEM((S * L, 4 * C), f32),
            pltpu.VMEM((D, 4 * C), bf),
            pltpu.VMEM((X, 2, S * L, C), bf),
            pltpu.VMEM((D // 128, 128), bf),
            pltpu.VMEM((1, D), f32),
            pltpu.VMEM((CORES, S, H, BL), f32),
            pltpu.VMEM((4, S, C), bf),
            pltpu.VMEM((S, H), f32),
            pltpu.VMEM((1, S * L), f32),
            pltpu.VMEM((far, 1, S * L), f32),
            pltpu.VMEM((S, CORES, C, C), bf),
            pltpu.VMEM((X, S, CORES, L, C), f32),
            pltpu.VMEM((CORES, 3, S, C), f32),
            pltpu.VMEM((CORES, Z, 3, S, C), f32),
            dma((S * L // R,)), dma, dma, dma((4,)), regular((max(Z - 2, 1),)), regular,
            dma((far,)), dma((far, 5)), dma((far,)), dma((far,)), dma((3,)), dma((3,)),
            dma, dma, dma((CORES,)), dma((CORES,)),
        ],
        compiler_params=pltpu.CompilerParams(
            collective_id=0, has_side_effects=True, vmem_limit_bytes=56 * 1024 * 1024
        ),
    )(
        tokens.reshape(S * L, D),
        norm_gain.reshape(D // 128, 128),
        key_weight,
        value_weight,
        jnp.transpose(cum_gates, (0, 2, 1)),
        new_query,
        new_key,
        new_value,
        new_gate,
    )
    return pl.pallas_call(
        write_out,
        out_shape=tuple(jax.ShapeDtypeStruct(r.shape, r.dtype) for r in results),
        in_specs=[vmem] * 3,
        out_specs=(hbm, hbm, hbm),
        scratch_shapes=[dma((3,))],
    )(*(pltpu.with_memory_space_constraint(r, pltpu.VMEM) for r in results))


def solution(mesh):
    in_specs = (
        P("gr", ("sp", "tp"), None),
        P(),
        P(None, "tp"),
        P(None, "tp"),
        P("gr", "sp", "tp"),
        P("gr", "tp"),
        P("gr", "tp"),
        P("gr", "tp"),
        P("gr", "tp"),
    )
    out_specs = (P("gr", "sp", "tp"), P("gr", "sp", "tp"), P("gr", "tp"))
    return jax.shard_map(body, mesh=mesh, in_specs=in_specs, out_specs=out_specs, check_vma=False)
```

```python
import functools

import jax
import jax.numpy as jnp
from jax import lax
from jax.experimental import pallas as pl
from jax.experimental.pallas import tpu as pltpu
from jax.sharding import PartitionSpec as P

HD = 64
CORES = 2
LEAD = 4
EXTRA = 8
RAW = 2

epsilon = 1e-06
masked_score = -1e30
MESH = pl.DeviceIdType.MESH


def kernel(
    dims,
    tok_hbm, gain_hbm, wk_hbm, wv_hbm, gates_hbm, q_hbm, nk_hbm, nv_hbm, ng_hbm,
    kbuf, vbuf, ro_ref,
    tok, raw, inv, nb, rx, acc, wbuf, ybuf, gain_v, gain_row, gates_v, new_v, ng_v,
    inv_tx, inv_rx, qblock, gate_rep, stats_tx, stats_rx, lent, lent_tx, lent_rx,
    loc_sem, raw_sem, w_sem, small_sem, hop_sem, answer_sem, ready_sem,
    sx_sem, rx_sem, si_sem, ri_sem, sw_sem, rw_sem, sy_sem, ry_sem, sz_sem, rz_sem,
    sl_sem, rl_sem, sf_sem, rf_sem, sg_sem, rg_sem, sk_sem, rk_sem,
):
    S, L, R, T, Z = dims
    X = T // CORES
    f32, bf = jnp.float32, jnp.bfloat16
    rows_each, D = tok.shape
    NC, KC = nb.shape[0], nb.shape[2]
    blocks = rows_each // R
    C = kbuf.shape[2]
    H = C // HD
    BL = T * L
    E = EXTRA
    kept = rows_each - E
    tp = lax.axis_index("tp")
    z = lax.axis_index("sp")
    x, c = tp // CORES, tp % CORES
    lender, helper = z == Z - 1, z == 0
    if Z == 1:
        lender = helper = z < 0
    partner = x * CORES + (CORES - 1 - c)

    def peer(d):
        return {"tp": ((x + d) % X) * CORES + c}

    def rows(j):
        return pl.ds(j * R, R)

    first = [pltpu.make_async_copy(tok_hbm.at[:, pl.ds(k * KC, KC)], raw.at[k], raw_sem) for k in range(RAW)]
    for copy in first:
        copy.start()
    rx[:, :, kept:, :] = jnp.zeros((rx.shape[0], NC, 2 * E, KC), bf)
    barrier = pltpu.get_barrier_semaphore()
    for d in range(1, X):
        pl.semaphore_signal(barrier, inc=1, device_id=peer(d), device_id_type=MESH)
    sides = (z > 0).astype(jnp.int32) + (z < Z - 1).astype(jnp.int32)

    def greet_sides(sem):
        @pl.when(z > 0)
        def _():
            pl.semaphore_signal(sem, inc=1, device_id={"sp": z - 1}, device_id_type=MESH)

        @pl.when(z < Z - 1)
        def _():
            pl.semaphore_signal(sem, inc=1, device_id={"sp": z + 1}, device_id_type=MESH)

    @pl.when(z < Z - 1)
    def _():
        pl.semaphore_signal(barrier, inc=1, device_id={"sp": z + 1}, device_id_type=MESH)

    pl.semaphore_signal(barrier, inc=1, device_id={"tp": partner}, device_id_type=MESH)

    loads = [pltpu.make_async_copy(tok_hbm.at[rows(j)], tok.at[rows(j)], loc_sem.at[j]) for j in range(blocks)]
    small = [
        pltpu.make_async_copy(src, dst, small_sem.at[min(i, 3)])
        for i, (src, dst) in enumerate(
            [(gain_hbm, gain_v), (gates_hbm, gates_v.at[0]), (ng_hbm, ng_v), (q_hbm, new_v.at[0]), (nk_hbm, new_v.at[1]), (nv_hbm, new_v.at[2])]
        )
    ]
    for copy in loads:
        copy.start()
    for copy in small:
        copy.start()
    w_copies = [
        pltpu.make_async_copy(src, wbuf.at[:, pl.ds(2 * i * C, C)], w_sem) for i, src in enumerate((wk_hbm, wv_hbm))
    ]

    def to_partner(src, dst, i):
        return pltpu.make_async_remote_copy(
            src, dst, sw_sem.at[i], rw_sem.at[i], device_id={"tp": partner}, device_id_type=MESH
        )

    shares = [
        to_partner(wk_hbm, wbuf.at[:, pl.ds(C, C)], 0),
        to_partner(wv_hbm, wbuf.at[:, pl.ds(3 * C, C)], 0),
        to_partner(gates_hbm, gates_v.at[1], 1),
        to_partner(q_hbm, new_v.at[3], 2),
    ]
    both_weights = to_partner(wbuf.at[:, pl.ds(0, 2 * C)], wbuf.at[:, pl.ds(0, 2 * C)], 0)

    HALF = NC // 2

    def x_copy(d, k, count=rows_each):
        return pltpu.make_async_remote_copy(
            raw.at[k] if k < RAW else nb.at[k, pl.ds(0, count)],
            rx.at[d - 1, k, pl.ds(0, count)],
            sx_sem.at[d - 1, (k >= RAW) + (k >= LEAD)],
            rx_sem.at[d - 1, k],
            device_id=peer(d),
            device_id_type=MESH,
        )

    def x_sent(d, first, stop, group, count=rows_each):
        part = rx.at[d - 1, pl.ds(first, stop - first), pl.ds(0, count)]
        return pltpu.make_async_remote_copy(
            part, part, sx_sem.at[d - 1, group], rx_sem.at[d - 1, 0], device_id=peer(d), device_id_type=MESH
        )

    def x_arrival(d, k, count=rows_each):
        part = rx.at[d - 1, k, pl.ds(0, count)]
        return pltpu.make_async_remote_copy(
            part, part, sx_sem.at[d - 1, 0], rx_sem.at[d - 1, k], device_id=peer(d), device_id_type=MESH
        )

    def by_block(act):
        pl.when(lender)(lambda: act(kept))
        pl.when(jnp.logical_not(lender))(lambda: act(rows_each))

    def to_block(src, dst, send_sem, recv_sem, block, target):
        return pltpu.make_async_remote_copy(
            src, dst, send_sem, recv_sem, device_id={"sp": block, "tp": target}, device_id_type=MESH
        )

    lend = to_block(nb.at[:, pl.ds(kept, E)], lent, sl_sem, rl_sem, 0, tp)

    def forward(d):
        return pltpu.make_async_remote_copy(
            lent, rx.at[d - 1, :, pl.ds(rows_each, E)], sf_sem.at[d - 1], rf_sem.at[d - 1],
            device_id=peer(d), device_id_type=MESH,
        )

    def gate_copy(d, g):
        return to_block(
            gate_rep.at[d, S - 1, g, pl.ds(L - E, E)], gate_rep.at[d, S - 1, g, pl.ds(L, E)],
            sg_sem.at[d - 1, g], rg_sem.at[d - 1, g], 0, tp,
        )

    def give_back(d, g):
        return to_block(
            lent_tx.at[d - 1, g], lent_rx.at[d - 1, g], sk_sem.at[d - 1, g], rk_sem.at[d - 1, g],
            Z - 1, partner if g else tp,
        )

    def inv_copy(d):
        return pltpu.make_async_remote_copy(
            inv_tx, inv_rx.at[d - 1], si_sem.at[d - 1], ri_sem.at[d - 1], device_id=peer(d), device_id_type=MESH
        )

    def norm(v, r, k):
        return (v.astype(f32) * r * gain_row[:, pl.ds(k * KC, KC)]).astype(bf)

    pltpu.make_async_copy(raw, raw, raw_sem).wait()
    before = (z > 0).astype(jnp.int32)
    pl.semaphore_wait(barrier, 1 + (X - 1) + before)

    def send(chunks, count=rows_each):
        for k in chunks:
            for d in range(1, X):
                x_copy(d, k, count).start()

    send(range(RAW))

    @pl.when(z > 0)
    def _():
        pl.semaphore_signal(answer_sem, inc=1, device_id={"sp": z - 1}, device_id_type=MESH)


    small[0].wait()
    g = gain_v[...].astype(f32)
    lanes = g.shape[1]
    for i in range(g.shape[0]):
        gain_row[:, pl.ds(i * lanes, lanes)] = g[i : i + 1, :]
    for j in range(blocks):
        loads[j].wait()
        v = tok[rows(j), :].astype(f32)
        r = lax.rsqrt(jnp.mean(v * v, axis=-1, keepdims=True) + epsilon)
        inv[rows(j), :] = jnp.broadcast_to(r, (R, KC))
    for copy in w_copies:
        copy.start()
    eye = lax.broadcasted_iota(jnp.int32, (rows_each, rows_each), 0) == lax.broadcasted_iota(
        jnp.int32, (rows_each, rows_each), 1
    )
    inv_tx[...] = jnp.sum(jnp.where(eye, inv[:, :rows_each], 0.0), axis=0, keepdims=True)
    for k in range(RAW, NC):
        nb[k] = norm(tok[:, pl.ds(k * KC, KC)], inv[...], k)
        if k < LEAD:
            by_block(lambda count: send([k], count))
        if k == RAW:
            for d in range(1, X):
                inv_copy(d).start()
        if k == HALF - 1:
            pl.when(c == 0)(lambda: by_block(lambda count: send(range(LEAD, HALF), count)))
    for copy in shares[2:] + shares[:2]:
        copy.start()
    for k in range(RAW):
        nb[k] = norm(raw[k], inv[...], k)
    pl.when(z < Z - 1)(lambda: pl.semaphore_wait(answer_sem, 1))
    for r in range(Z - 2):
        greet_sides(hop_sem.at[r])
        pl.semaphore_wait(hop_sem.at[r], sides)
    pl.when(lender)(lend.start)

    @pl.when(c != 0)
    def _():
        for d in range(1, X):
            x_sent(d, 0, RAW, 0).wait_send()
            by_block(lambda count: x_sent(d, RAW, LEAD, 1, count).wait_send())

    small[1].wait()
    small[2].wait()
    pltpu.make_async_copy(new_v.at[pl.ds(0, 3)], new_v.at[pl.ds(0, 3)], small_sem.at[3]).wait()
    for i in (2, 3):
        shares[i].wait_recv()

    scale = HD ** (-0.5)
    lane_head = lax.broadcasted_iota(jnp.int32, (C, C), 1) // HD
    same_head = lane_head == lax.broadcasted_iota(jnp.int32, (C, C), 0) // HD
    diagonal = lax.broadcasted_iota(jnp.int32, (C, C), 0) == lax.broadcasted_iota(jnp.int32, (C, C), 1)
    own_head = lax.broadcasted_iota(jnp.int32, (H, C), 1) // HD == lax.broadcasted_iota(jnp.int32, (H, C), 0)
    heads_eye = lax.broadcasted_iota(jnp.int32, (H, H), 0) == lax.broadcasted_iota(jnp.int32, (H, H), 1)
    last_block = z == Z - 1

    def as_row(column):
        return jnp.sum(jnp.where(own_head, column, 0.0), axis=0, keepdims=True)

    def source(d):
        return ((x + X - d) % X) * CORES + c

    for s in range(S):
        for g in range(CORES):
            column = jnp.sum(jnp.where(diagonal, new_v[3 * g, s : s + 1, :].astype(f32), 0.0), axis=1, keepdims=True)
            qblock[s, g] = jnp.where(same_head, column, 0.0).astype(bf)
    head_of_lane = lax.broadcasted_iota(jnp.int32, (L, C), 1) // HD
    for d in range(X):
        pick = lax.broadcasted_iota(jnp.int32, (L, BL), 1) == lax.broadcasted_iota(
            jnp.int32, (L, BL), 0
        ) + source(d) * L
        for s in range(S):
            for g in range(CORES):
                spread = jnp.zeros((L, C), f32)
                for h in range(H):
                    column = jnp.sum(jnp.where(pick, gates_v[g, s, h : h + 1, :], 0.0), axis=1, keepdims=True)
                    spread = jnp.where(head_of_lane == h, column, spread)
                gate_rep[d, s, g, :L] = spread

                @pl.when(jnp.logical_not(helper))
                def _():
                    gate_rep[d, s, g, L:] = jnp.full((E, C), -masked_score, f32)

    for s in range(S):
        fresh = jnp.dot(new_v[1, s : s + 1, :], qblock[s, 0], preferred_element_type=f32) * scale
        own_gate = jnp.sum(jnp.where(heads_eye, ng_v[s : s + 1, :], 0.0), axis=1, keepdims=True)
        fresh = jnp.where(last_block, fresh - as_row(gates_v[0, s, :, BL - 1 : BL] + own_gate), masked_score)
        weight = jnp.where(last_block, jnp.ones_like(fresh), 0.0)
        stats_tx[0, 0, s : s + 1, :] = fresh
        stats_tx[0, 1, s : s + 1, :] = weight
        stats_tx[0, 2, s : s + 1, :] = weight * new_v[2, s : s + 1, :].astype(f32)
        stats_tx[1, 0, s : s + 1, :] = jnp.full((1, C), masked_score, f32)
        stats_tx[1, 1, s : s + 1, :] = jnp.zeros((1, C), f32)
        stats_tx[1, 2, s : s + 1, :] = jnp.zeros((1, C), f32)

    pl.when(c != 0)(lambda: by_block(lambda count: send(range(LEAD, HALF), count)))
    for d in range(1, X):
        for g in range(CORES):
            pl.when(lender)(gate_copy(d, g).start)
    for d in range(1, X):
        inv_copy(d).wait_recv()
        r = jnp.sum(jnp.where(eye, inv_rx[d - 1], 0.0), axis=1, keepdims=True)
        for k in range(RAW):
            x_arrival(d, k).wait_recv()
            rx[d - 1, k, :rows_each] = norm(rx[d - 1, k, :rows_each], r, k)

    def w_part(k):
        return wbuf[pl.ds(k * KC if isinstance(k, int) else pl.multiple_of(k * KC, KC), KC), :]

    def y_copy(d, s, v):
        at = pl.ds(pl.multiple_of(source(d) * L, L), L)
        return pltpu.make_async_remote_copy(
            ybuf.at[d, v, pl.ds(s * L, L)], (kbuf, vbuf)[v].at[s, at],
            sy_sem, ry_sem, device_id={"tp": partner}, device_id_type=MESH,
        )

    def rows_of(d, s):
        return L + E if d and s == S - 1 else L

    def finish(d, y, last):
        pairs = [(g, s) for g in range(CORES) for s in range(S)]
        before = {(g, s): [stats_tx[g, i, s : s + 1, :] for i in range(3)] for g, s in pairs}
        scores = {}
        for g, s in pairs:
            stop = rows_of(d, s)
            keys = y[s * L : s * L + stop, g * C : (g + 1) * C]
            scores[g, s] = jnp.dot(keys, qblock[s, g], preferred_element_type=f32) * scale - gate_rep[d, s, g, :stop]
        after = {}
        for g, s in pairs:
            old_top, old_total, old_weighted = before[g, s]
            values = y[s * L : s * L + rows_of(d, s), (2 + g) * C : (3 + g) * C].astype(f32)
            top = jnp.maximum(jnp.max(scores[g, s], axis=0, keepdims=True), old_top)
            weights = jnp.exp(scores[g, s] - top)
            factor = jnp.exp(old_top - top)
            total = jnp.sum(weights, axis=0, keepdims=True) + factor * old_total
            weighted = jnp.sum(weights * values, axis=0, keepdims=True) + factor * old_weighted
            after[g, s] = (top, total, weighted)
        for g, s in pairs:
            for i, row in enumerate(after[g, s]):
                stats_tx[g, i, s : s + 1, :] = row
        if last:
            for s in range(S):
                for i, row in enumerate(after[0, s]):
                    stats_rx[0, z, i, s : s + 1, :] = row

    def deliver(d, y):
        place = pl.ds(pl.multiple_of(source(d) * L, L), L)
        for s in range(S):
            part = y[s * L : (s + 1) * L]
            kbuf[s, place, :] = part[:, :C]
            vbuf[s, place, :] = part[:, 2 * C : 3 * C]
        ybuf[d, 0] = y[:rows_each, C : 2 * C]
        ybuf[d, 1] = y[:rows_each, 3 * C :]

    def send_partner(d):
        for s in range(S):
            for v in range(2):
                y_copy(d, s, v).start()

    pltpu.make_async_copy(wbuf.at[:, pl.ds(0, 2 * C)], wbuf.at[:, pl.ds(0, 2 * C)], w_sem).wait()
    both_weights.wait_recv()

    @pl.when(helper)
    def _():
        to_block(lent, lent, sl_sem, rl_sem, 0, tp).wait_recv()
        for d in range(1, X):
            forward(d).start()

    by_block(lambda count: send(range(HALF, NC), count))
    acc[...] = jnp.zeros_like(acc)

    def near(k, carry):
        acc[:rows_each] += jnp.dot(nb[k], w_part(k), preferred_element_type=f32)
        return carry

    lax.fori_loop(0, NC, near, 0)
    y = acc[:rows_each].astype(bf)
    deliver(0, y)
    finish(0, y, X == 1)
    send_partner(0)
    pl.semaphore_signal(ready_sem, inc=1, device_id={"tp": partner}, device_id_type=MESH)
    for d in range(1, X):
        for g in range(CORES):

            @pl.when(lender)
            def _(d=d, g=g):
                gate_copy(d, g).wait_send()
                gate_rep[d, S - 1, g, L - E : L] = jnp.full((E, C), -masked_score, f32)

            pl.when(helper)(gate_copy(d, g).wait_recv)
    pl.semaphore_wait(ready_sem, 1)

    for d in range(1, X):
        acc[...] = jnp.zeros_like(acc)

        def far(k, carry, d=d):
            acc[...] += jnp.dot(rx[d - 1, k], w_part(k), preferred_element_type=f32)
            return carry

        def far_arriving(k, carry, d=d):
            by_block(lambda count: x_arrival(d, k, count).wait_recv())
            return far(k, carry, d)

        pl.when(helper)(forward(d).wait_recv)
        lax.fori_loop(0, RAW, far, 0)
        lax.fori_loop(RAW, NC - 1, far_arriving, 0)
        by_block(lambda count: x_arrival(d, NC - 1, count).wait_recv())
        y = (acc[...] + jnp.dot(rx[d - 1, NC - 1], w_part(NC - 1), preferred_element_type=f32)).astype(bf)

        @pl.when(helper)
        def _(d=d, y=y):
            for g in range(CORES):
                for v in range(2):
                    lent_tx[d - 1, g, v] = y[rows_each:, (2 * v + g) * C : (2 * v + g + 1) * C]
                give_back(d, g).start()

        if d < X - 1:
            deliver(d, y)
            finish(d, y, False)
            send_partner(d)
        else:
            finish(d, y, True)

    def z_target(i):
        return jnp.where(2 * z >= Z, i, Z - 1 - i)

    def z_copy(i, other):
        to = z_target(i)
        return pltpu.make_async_remote_copy(
            stats_tx.at[other], stats_rx.at[other, z], sz_sem.at[other], rz_sem.at[other],
            device_id={"sp": to, "tp": partner if other else tp}, device_id_type=MESH,
        )

    for i in range(Z):
        for first_core in range(CORES):

            @pl.when(c == first_core)
            def _(i=i, first_core=first_core):
                for core in range(CORES):
                    if core == first_core:
                        pl.when(z_target(i) != z)(z_copy(i, 0).start)
                    else:
                        z_copy(i, 1).start()

    if X > 1:
        deliver(X - 1, y)
        send_partner(X - 1)
    for d in range(1, X):
        inv_copy(d).wait_send()
        pl.when(c == 0)(x_sent(d, 0, RAW, 0).wait_send)
        pl.when(c == 0)(lambda: by_block(lambda count: x_sent(d, RAW, LEAD, 1, count).wait_send()))
        by_block(lambda count: x_sent(d, LEAD, NC, 2, count).wait_send())

        @pl.when(helper)
        def _(d=d):
            forward(d).wait_send()
            for g in range(CORES):
                give_back(d, g).wait_send()

    pl.when(lender)(lend.wait_send)
    both_weights.wait_send()
    shares[2].wait_send()
    shares[3].wait_send()
    halves = pltpu.make_async_remote_copy(ybuf, ybuf, sy_sem, ry_sem, device_id={"tp": partner}, device_id_type=MESH)
    halves.wait_send()
    halves.wait_recv()

    def z_whole(other):
        part = stats_rx.at[other, pl.ds(0, Z - 1 + other)]
        return pltpu.make_async_remote_copy(
            part, part, sz_sem.at[other], rz_sem.at[other],
            device_id={"tp": partner if other else tp}, device_id_type=MESH,
        )

    for other in range(CORES):
        if Z - 1 + other:
            z_whole(other).wait_recv()

    @pl.when(lender)
    def _():
        for d in range(1, X):
            for g in range(CORES):
                give_back(d, g).wait_recv()
                core = CORES - 1 - c if g else c
                at = pl.ds(pl.multiple_of(((x + X - d) % X * CORES + core) * L + L - E, E), E)
                kbuf[S - 1, at, :] = lent_rx[d - 1, g, 0]
                vbuf[S - 1, at, :] = lent_rx[d - 1, g, 1]

    entries = [(i, other) for i in range(Z) for other in range(CORES)]
    tops = [stats_rx[other, i, 0] for i, other in entries]
    most = functools.reduce(jnp.maximum, tops)
    factors = [jnp.exp(top - most) for top in tops]
    total = functools.reduce(jnp.add, [f * stats_rx[other, i, 1] for f, (i, other) in zip(factors, entries)])
    weighted = functools.reduce(jnp.add, [f * stats_rx[other, i, 2] for f, (i, other) in zip(factors, entries)])
    ro_ref[...] = (weighted / total).astype(ro_ref.dtype)
    for other in range(CORES):
        if Z - 1 + other:
            z_whole(other).wait_send()


def scoped(dims, semaphores, *refs):
    pl.run_scoped(lambda *held: kernel(dims, *refs, *held), *semaphores)


def write_out(*refs):
    sems = refs[-1]
    count = (len(refs) - 1) // 2
    copies = [pltpu.make_async_copy(refs[i], refs[count + i], sems.at[i]) for i in range(count)]
    for copy in copies:
        copy.start()
    for copy in copies:
        copy.wait()


def body(
    tokens, norm_gain, key_weight, value_weight, cum_gates, new_query, new_key, new_value, new_gate
):
    S, L, D = tokens.shape
    C = key_weight.shape[1]
    H = C // HD
    T = lax.axis_size("tp")
    Z = lax.axis_size("sp")
    X = T // CORES
    BL = T * L
    R = 32 if L % 32 == 0 else L
    KC = 256 if D % 256 == 0 else D // 2
    NC = D // KC
    bf, f32 = jnp.bfloat16, jnp.float32
    hbm = pl.BlockSpec(memory_space=pltpu.HBM)
    dma = pltpu.SemaphoreType.DMA
    regular = pltpu.SemaphoreType.REGULAR
    far = max(X - 1, 1)
    vmem = pl.BlockSpec(memory_space=pltpu.VMEM)
    semaphores = [
        dma((S * L // R,)), dma, dma, dma((4,)), regular((max(Z - 2, 1),)), regular, regular,
        dma((far, 3)), dma((far, NC)), dma((far,)), dma((far,)), dma((3,)), dma((3,)),
        dma, dma, dma((CORES,)), dma((CORES,)),
        dma, dma, dma((far,)), dma((far,)),
        dma((far, CORES)), dma((far, CORES)), dma((far, CORES)), dma((far, CORES)),
    ]
    results = pl.pallas_call(
        functools.partial(scoped, (S, L, R, T, Z), semaphores),
        out_shape=(
            pltpu.VMEM((S, BL, C), bf),
            pltpu.VMEM((S, BL, C), bf),
            pltpu.VMEM((S, C), bf),
        ),
        in_specs=[hbm] * 9,
        out_specs=(vmem, vmem, vmem),
        scratch_shapes=[
            pltpu.VMEM((S * L, D), bf),
            pltpu.VMEM((RAW, S * L, KC), bf),
            pltpu.VMEM((S * L, KC), f32),
            pltpu.VMEM((NC, S * L, KC), bf),
            pltpu.VMEM((far, NC, S * L + EXTRA, KC), bf),
            pltpu.VMEM((S * L + EXTRA, 4 * C), f32),
            pltpu.VMEM((D, 4 * C), bf),
            pltpu.VMEM((X, 2, S * L, C), bf),
            pltpu.VMEM((D // 128, 128), bf),
            pltpu.VMEM((1, D), f32),
            pltpu.VMEM((CORES, S, H, BL), f32),
            pltpu.VMEM((4, S, C), bf),
            pltpu.VMEM((S, H), f32),
            pltpu.VMEM((1, S * L), f32),
            pltpu.VMEM((far, 1, S * L), f32),
            pltpu.VMEM((S, CORES, C, C), bf),
            pltpu.VMEM((X, S, CORES, L + EXTRA, C), f32),
            pltpu.VMEM((CORES, 3, S, C), f32),
            pltpu.VMEM((CORES, Z, 3, S, C), f32),
            pltpu.VMEM((NC, EXTRA, KC), bf),
            pltpu.VMEM((far, CORES, 2, EXTRA, C), bf),
            pltpu.VMEM((far, CORES, 2, EXTRA, C), bf),
        ],
        compiler_params=pltpu.CompilerParams(
            collective_id=0, has_side_effects=True, vmem_limit_bytes=56 * 1024 * 1024
        ),
    )(
        tokens.reshape(S * L, D),
        norm_gain.reshape(D // 128, 128),
        key_weight,
        value_weight,
        jnp.transpose(cum_gates, (0, 2, 1)),
        new_query,
        new_key,
        new_value,
        new_gate,
    )
    return pl.pallas_call(
        write_out,
        out_shape=tuple(jax.ShapeDtypeStruct(r.shape, r.dtype) for r in results),
        in_specs=[vmem] * 3,
        out_specs=(hbm, hbm, hbm),
        scratch_shapes=[dma((3,))],
    )(*(pltpu.with_memory_space_constraint(r, pltpu.VMEM) for r in results))


def solution(mesh):
    in_specs = (
        P("gr", ("sp", "tp"), None),
        P(),
        P(None, "tp"),
        P(None, "tp"),
        P("gr", "sp", "tp"),
        P("gr", "tp"),
        P("gr", "tp"),
        P("gr", "tp"),
        P("gr", "tp"),
    )
    out_specs = (P("gr", "sp", "tp"), P("gr", "sp", "tp"), P("gr", "tp"))
    return jax.shard_map(body, mesh=mesh, in_specs=in_specs, out_specs=out_specs, check_vma=False)
```

```python
import functools

import jax
import jax.numpy as jnp
from jax import lax
from jax.experimental import pallas as pl
from jax.experimental.pallas import tpu as pltpu
from jax.sharding import PartitionSpec as P

HD = 64
CORES = 2
LEAD = 4
TAIL = 4
EXTRA, SLOTS = 8, 2
RAW = 2

epsilon = 1e-06
masked_score = -1e30
MESH = pl.DeviceIdType.MESH


def kernel(
    dims,
    tok_hbm, gain_hbm, wk_hbm, wv_hbm, gates_hbm, q_hbm, nk_hbm, nv_hbm, ng_hbm,
    kbuf, vbuf, ro_ref,
    tok, raw, inv, nb, rx, acc, wbuf, ybuf, gain_v, gain_row, gates_v, new_v, ng_v,
    inv_tx, inv_rx, qblock, gate_rep, stats_tx, stats_rx, lent, lent_tx, lent_rx,
    loc_sem, raw_sem, w_sem, small_sem, hop_sem, answer_sem, ready_sem,
    sx_sem, rx_sem, si_sem, ri_sem, sw_sem, rw_sem, sy_sem, ry_sem, sz_sem, rz_sem,
    sl_sem, rl_sem, sf_sem, rf_sem, sg_sem, rg_sem, sk_sem, rk_sem,
):
    S, L, R, T, Z = dims
    X = T // CORES
    f32, bf = jnp.float32, jnp.bfloat16
    rows_each, D = tok.shape
    NC, KC = nb.shape[0], nb.shape[2]
    blocks = rows_each // R
    C = kbuf.shape[2]
    H = C // HD
    BL = T * L
    E, EE = EXTRA, SLOTS * EXTRA
    kept = rows_each - E
    tp = lax.axis_index("tp")
    z = lax.axis_index("sp")
    x, c = tp // CORES, tp % CORES
    slots = [j for j in range(SLOTS) if Z - 1 - j > 0]

    def lends(j, core):
        return jnp.logical_and(z == Z - 1 - j, core >= j)

    def helps(j, core):
        return jnp.logical_and(z == 0, core >= j)

    lender = functools.reduce(jnp.logical_or, [lends(j, c) for j in slots], z < 0)
    pauses = c != 0
    partner = x * CORES + (CORES - 1 - c)

    def peer(d):
        return {"tp": ((x + d) % X) * CORES + c}

    def rows(j):
        return pl.ds(j * R, R)

    first = [pltpu.make_async_copy(tok_hbm.at[:, pl.ds(k * KC, KC)], raw.at[k], raw_sem) for k in range(RAW)]
    for copy in first:
        copy.start()
    rx[:, :, kept:, :] = jnp.zeros((rx.shape[0], NC, E + EE, KC), bf)
    barrier = pltpu.get_barrier_semaphore()
    for d in range(1, X):
        pl.semaphore_signal(barrier, inc=1, device_id=peer(d), device_id_type=MESH)
    sides = (z > 0).astype(jnp.int32) + (z < Z - 1).astype(jnp.int32)

    def greet_sides(sem):
        @pl.when(z > 0)
        def _():
            pl.semaphore_signal(sem, inc=1, device_id={"sp": z - 1}, device_id_type=MESH)

        @pl.when(z < Z - 1)
        def _():
            pl.semaphore_signal(sem, inc=1, device_id={"sp": z + 1}, device_id_type=MESH)

    @pl.when(z < Z - 1)
    def _():
        pl.semaphore_signal(barrier, inc=1, device_id={"sp": z + 1}, device_id_type=MESH)

    pl.semaphore_signal(barrier, inc=1, device_id={"tp": partner}, device_id_type=MESH)

    loads = [pltpu.make_async_copy(tok_hbm.at[rows(j)], tok.at[rows(j)], loc_sem.at[j]) for j in range(blocks)]
    small = [
        pltpu.make_async_copy(src, dst, small_sem.at[min(i, 3)])
        for i, (src, dst) in enumerate(
            [(gain_hbm, gain_v), (gates_hbm, gates_v.at[0]), (ng_hbm, ng_v), (q_hbm, new_v.at[0]), (nk_hbm, new_v.at[1]), (nv_hbm, new_v.at[2])]
        )
    ]
    for copy in loads:
        copy.start()
    for copy in small:
        copy.start()
    w_copies = [
        pltpu.make_async_copy(src, wbuf.at[:, pl.ds(2 * i * C, C)], w_sem) for i, src in enumerate((wk_hbm, wv_hbm))
    ]

    def to_partner(src, dst, i):
        return pltpu.make_async_remote_copy(
            src, dst, sw_sem.at[i], rw_sem.at[i], device_id={"tp": partner}, device_id_type=MESH
        )

    shares = [
        to_partner(wk_hbm, wbuf.at[:, pl.ds(C, C)], 0),
        to_partner(wv_hbm, wbuf.at[:, pl.ds(3 * C, C)], 0),
        to_partner(gates_hbm, gates_v.at[1], 1),
        to_partner(q_hbm, new_v.at[3], 2),
    ]
    both_weights = to_partner(wbuf.at[:, pl.ds(0, 2 * C)], wbuf.at[:, pl.ds(0, 2 * C)], 0)

    HALF = NC // 2

    def x_copy(d, k, count=rows_each):
        return pltpu.make_async_remote_copy(
            raw.at[k] if k < RAW else nb.at[k, pl.ds(0, count)],
            rx.at[d - 1, k, pl.ds(0, count)],
            sx_sem.at[d - 1, (k >= RAW) + (k >= LEAD)],
            rx_sem.at[d - 1, k],
            device_id=peer(d),
            device_id_type=MESH,
        )

    def x_sent(d, first, stop, group, count=rows_each):
        part = rx.at[d - 1, pl.ds(first, stop - first), pl.ds(0, count)]
        return pltpu.make_async_remote_copy(
            part, part, sx_sem.at[d - 1, group], rx_sem.at[d - 1, 0], device_id=peer(d), device_id_type=MESH
        )

    cut, split = (S - 1) * L, NC - TAIL

    def x_part(d, k, part, count=rows_each):
        at = pl.ds(cut, count - cut) if part else pl.ds(0, cut)
        return pltpu.make_async_remote_copy(
            nb.at[k, at], rx.at[d - 1, k, at], sx_sem.at[d - 1, 2], rx_sem.at[d - 1, k + TAIL * part],
            device_id=peer(d), device_id_type=MESH,
        )

    def x_arrival(d, k, count=rows_each):
        part = rx.at[d - 1, k, pl.ds(0, count)]
        return pltpu.make_async_remote_copy(
            part, part, sx_sem.at[d - 1, 0], rx_sem.at[d - 1, k], device_id=peer(d), device_id_type=MESH
        )

    def by_block(act):
        pl.when(lender)(lambda: act(kept))
        pl.when(jnp.logical_not(lender))(lambda: act(rows_each))

    def to_block(src, dst, send_sem, recv_sem, block, target):
        return pltpu.make_async_remote_copy(
            src, dst, send_sem, recv_sem, device_id={"sp": block, "tp": target}, device_id_type=MESH
        )

    def lend(j):
        return to_block(nb.at[:, pl.ds(kept, E)], lent.at[j], sl_sem.at[j], rl_sem.at[j], 0, tp)

    def forward(d, j):
        return pltpu.make_async_remote_copy(
            lent.at[j], rx.at[d - 1, :, pl.ds(rows_each + j * E, E)], sf_sem.at[d - 1, j], rf_sem.at[d - 1, j],
            device_id=peer(d), device_id_type=MESH,
        )

    def gate_copy(d, g, j):
        return to_block(
            gate_rep.at[d, S - 1, g, pl.ds(L - E, E)], gate_rep.at[d, S - 1, g, pl.ds(L + j * E, E)],
            sg_sem.at[d - 1, g, j], rg_sem.at[d - 1, g, j], 0, tp,
        )

    def give_back(d, g, j):
        return to_block(
            lent_tx.at[d - 1, g, j], lent_rx.at[d - 1, g], sk_sem.at[d - 1, g, j], rk_sem.at[d - 1, g, j],
            Z - 1 - j, partner if g else tp,
        )

    def inv_copy(d):
        return pltpu.make_async_remote_copy(
            inv_tx, inv_rx.at[d - 1], si_sem.at[d - 1], ri_sem.at[d - 1], device_id=peer(d), device_id_type=MESH
        )

    def norm(v, r, k):
        return (v.astype(f32) * r * gain_row[:, pl.ds(k * KC, KC)]).astype(bf)

    pltpu.make_async_copy(raw, raw, raw_sem).wait()
    before = (z > 0).astype(jnp.int32)
    pl.semaphore_wait(barrier, 1 + (X - 1) + before)

    def send(chunks, count=rows_each):
        for k in chunks:
            for d in range(1, X):
                x_copy(d, k, count).start()

    send(range(RAW))

    @pl.when(z > 0)
    def _():
        pl.semaphore_signal(answer_sem, inc=1, device_id={"sp": z - 1}, device_id_type=MESH)


    small[0].wait()
    g = gain_v[...].astype(f32)
    lanes = g.shape[1]
    for i in range(g.shape[0]):
        gain_row[:, pl.ds(i * lanes, lanes)] = g[i : i + 1, :]
    for j in range(blocks):
        loads[j].wait()
        v = tok[rows(j), :].astype(f32)
        r = lax.rsqrt(jnp.mean(v * v, axis=-1, keepdims=True) + epsilon)
        inv[rows(j), :] = jnp.broadcast_to(r, (R, KC))
    for copy in w_copies:
        copy.start()
    eye = lax.broadcasted_iota(jnp.int32, (rows_each, rows_each), 0) == lax.broadcasted_iota(
        jnp.int32, (rows_each, rows_each), 1
    )
    inv_tx[...] = jnp.sum(jnp.where(eye, inv[:, :rows_each], 0.0), axis=0, keepdims=True)
    for k in range(RAW, NC):
        nb[k] = norm(tok[:, pl.ds(k * KC, KC)], inv[...], k)
        if k < LEAD:
            by_block(lambda count: send([k], count))
        if k == RAW:
            for d in range(1, X):
                inv_copy(d).start()
        if k == HALF - 1:
            pl.when(jnp.logical_not(pauses))(lambda: by_block(lambda count: send(range(LEAD, HALF), count)))
    for copy in shares[2:] + shares[:2]:
        copy.start()
    for k in range(RAW):
        nb[k] = norm(raw[k], inv[...], k)
    pl.when(z < Z - 1)(lambda: pl.semaphore_wait(answer_sem, 1))
    for r in range(Z - 2):
        greet_sides(hop_sem.at[r])
        pl.semaphore_wait(hop_sem.at[r], sides)
    for j in slots:
        pl.when(lends(j, c))(lend(j).start)

    @pl.when(pauses)
    def _():
        for d in range(1, X):
            x_sent(d, 0, RAW, 0).wait_send()
            by_block(lambda count: x_sent(d, RAW, LEAD, 1, count).wait_send())

    small[1].wait()
    small[2].wait()
    pltpu.make_async_copy(new_v.at[pl.ds(0, 3)], new_v.at[pl.ds(0, 3)], small_sem.at[3]).wait()
    for i in (2, 3):
        shares[i].wait_recv()

    scale = HD ** (-0.5)
    lane_head = lax.broadcasted_iota(jnp.int32, (C, C), 1) // HD
    same_head = lane_head == lax.broadcasted_iota(jnp.int32, (C, C), 0) // HD
    diagonal = lax.broadcasted_iota(jnp.int32, (C, C), 0) == lax.broadcasted_iota(jnp.int32, (C, C), 1)
    own_head = lax.broadcasted_iota(jnp.int32, (H, C), 1) // HD == lax.broadcasted_iota(jnp.int32, (H, C), 0)
    heads_eye = lax.broadcasted_iota(jnp.int32, (H, H), 0) == lax.broadcasted_iota(jnp.int32, (H, H), 1)
    last_block = z == Z - 1

    def as_row(column):
        return jnp.sum(jnp.where(own_head, column, 0.0), axis=0, keepdims=True)

    def source(d):
        return ((x + X - d) % X) * CORES + c

    for s in range(S):
        for g in range(CORES):
            column = jnp.sum(jnp.where(diagonal, new_v[3 * g, s : s + 1, :].astype(f32), 0.0), axis=1, keepdims=True)
            qblock[s, g] = jnp.where(same_head, column, 0.0).astype(bf)
    head_of_lane = lax.broadcasted_iota(jnp.int32, (L, C), 1) // HD
    for d in range(X):
        pick = lax.broadcasted_iota(jnp.int32, (L, BL), 1) == lax.broadcasted_iota(
            jnp.int32, (L, BL), 0
        ) + source(d) * L
        for s in range(S):
            for g in range(CORES):
                spread = jnp.zeros((L, C), f32)
                for h in range(H):
                    column = jnp.sum(jnp.where(pick, gates_v[g, s, h : h + 1, :], 0.0), axis=1, keepdims=True)
                    spread = jnp.where(head_of_lane == h, column, spread)
                gate_rep[d, s, g, :L] = spread

                for j in range(SLOTS):
                    theirs = helps(j, c) if j in slots else z < 0

                    @pl.when(jnp.logical_not(theirs))
                    def _(d=d, s=s, g=g, j=j):
                        gate_rep[d, s, g, L + j * E : L + (j + 1) * E] = jnp.full((E, C), -masked_score, f32)

    for s in range(S):
        fresh = jnp.dot(new_v[1, s : s + 1, :], qblock[s, 0], preferred_element_type=f32) * scale
        own_gate = jnp.sum(jnp.where(heads_eye, ng_v[s : s + 1, :], 0.0), axis=1, keepdims=True)
        fresh = jnp.where(last_block, fresh - as_row(gates_v[0, s, :, BL - 1 : BL] + own_gate), masked_score)
        weight = jnp.where(last_block, jnp.ones_like(fresh), 0.0)
        stats_tx[0, 0, s : s + 1, :] = fresh
        stats_tx[0, 1, s : s + 1, :] = weight
        stats_tx[0, 2, s : s + 1, :] = weight * new_v[2, s : s + 1, :].astype(f32)
        stats_tx[1, 0, s : s + 1, :] = jnp.full((1, C), masked_score, f32)
        stats_tx[1, 1, s : s + 1, :] = jnp.zeros((1, C), f32)
        stats_tx[1, 2, s : s + 1, :] = jnp.zeros((1, C), f32)

    pl.when(pauses)(lambda: by_block(lambda count: send(range(LEAD, HALF), count)))
    for d in range(1, X):
        for g in range(CORES):
            for j in slots:
                pl.when(lends(j, c))(gate_copy(d, g, j).start)
    for d in range(1, X):
        inv_copy(d).wait_recv()
        r = jnp.sum(jnp.where(eye, inv_rx[d - 1], 0.0), axis=1, keepdims=True)
        for k in range(RAW):
            x_arrival(d, k).wait_recv()
            rx[d - 1, k, :rows_each] = norm(rx[d - 1, k, :rows_each], r, k)

    def w_part(k):
        return wbuf[pl.ds(k * KC if isinstance(k, int) else pl.multiple_of(k * KC, KC), KC), :]

    def y_copy(d, s, v):
        at = pl.ds(pl.multiple_of(source(d) * L, L), L)
        return pltpu.make_async_remote_copy(
            ybuf.at[d, v, pl.ds(s * L, L)], (kbuf, vbuf)[v].at[s, at],
            sy_sem, ry_sem, device_id={"tp": partner}, device_id_type=MESH,
        )

    def rows_of(d, s):
        return L + EE if d and s == S - 1 else L

    def finish(d, y, first, prompts, last):
        pairs = [(g, s) for g in range(CORES) for s in prompts]
        before = {(g, s): [stats_tx[g, i, s : s + 1, :] for i in range(3)] for g, s in pairs}
        scores = {}
        for g, s in pairs:
            count = rows_of(d, s)
            keys = y[s * L - first : s * L - first + count, g * C : (g + 1) * C]
            scores[g, s] = jnp.dot(keys, qblock[s, g], preferred_element_type=f32) * scale - gate_rep[d, s, g, :count]
        after = {}
        for g, s in pairs:
            old_top, old_total, old_weighted = before[g, s]
            values = y[s * L - first : s * L - first + rows_of(d, s), (2 + g) * C : (3 + g) * C].astype(f32)
            top = jnp.maximum(jnp.max(scores[g, s], axis=0, keepdims=True), old_top)
            weights = jnp.exp(scores[g, s] - top)
            factor = jnp.exp(old_top - top)
            total = jnp.sum(weights, axis=0, keepdims=True) + factor * old_total
            weighted = jnp.sum(weights * values, axis=0, keepdims=True) + factor * old_weighted
            after[g, s] = (top, total, weighted)
        for g, s in pairs:
            for i, row in enumerate(after[g, s]):
                stats_tx[g, i, s : s + 1, :] = row
        if last:
            for s in prompts:
                for i, row in enumerate(after[0, s]):
                    stats_rx[0, z, i, s : s + 1, :] = row

    def deliver(d, y, first, prompts):
        place = pl.ds(pl.multiple_of(source(d) * L, L), L)
        for s in prompts:
            part = y[s * L - first : (s + 1) * L - first]
            kbuf[s, place, :] = part[:, :C]
            vbuf[s, place, :] = part[:, 2 * C : 3 * C]
            ybuf[d, 0, s * L : (s + 1) * L] = part[:, C : 2 * C]
            ybuf[d, 1, s * L : (s + 1) * L] = part[:, 3 * C :]

    def send_partner(d, prompts):
        for s in prompts:
            for v in range(2):
                y_copy(d, s, v).start()

    pltpu.make_async_copy(wbuf.at[:, pl.ds(0, 2 * C)], wbuf.at[:, pl.ds(0, 2 * C)], w_sem).wait()
    both_weights.wait_recv()

    for j in slots:

        @pl.when(helps(j, c))
        def _(j=j):
            lend(j).wait_recv()
            for d in range(1, X):
                forward(d, j).start()

    by_block(lambda count: send(range(HALF, split), count))
    for part in range(2):
        for k in range(split, NC):
            for d in range(1, X):
                by_block(lambda count: x_part(d, k, part, count).start())
    acc[...] = jnp.zeros_like(acc)

    def near(k, carry):
        acc[:rows_each] += jnp.dot(nb[k], w_part(k), preferred_element_type=f32)
        return carry

    lax.fori_loop(0, NC, near, 0)
    y = acc[:rows_each].astype(bf)
    deliver(0, y, 0, range(S))
    finish(0, y, 0, range(S), X == 1)
    send_partner(0, range(S))
    pl.semaphore_signal(ready_sem, inc=1, device_id={"tp": partner}, device_id_type=MESH)
    for d in range(1, X):
        for g in range(CORES):

            for j in slots:

                @pl.when(lends(j, c))
                def _(d=d, g=g, j=j):
                    gate_copy(d, g, j).wait_send()
                    gate_rep[d, S - 1, g, L - E : L] = jnp.full((E, C), -masked_score, f32)

                pl.when(helps(j, c))(gate_copy(d, g, j).wait_recv)
    pl.semaphore_wait(ready_sem, 1)

    for d in range(1, X):
        acc[...] = jnp.zeros_like(acc)

        def far(k, carry, d=d):
            acc[...] += jnp.dot(rx[d - 1, k], w_part(k), preferred_element_type=f32)
            return carry

        def far_arriving(k, carry, d=d):
            by_block(lambda count: x_arrival(d, k, count).wait_recv())
            return far(k, carry, d)

        for j in slots:
            pl.when(helps(j, c))(forward(d, j).wait_recv)
        lax.fori_loop(0, RAW, far, 0)
        lax.fori_loop(RAW, split, far_arriving, 0)
        last = d == X - 1
        if cut:
            for k in range(split, NC):
                x_part(d, k, 0).wait_recv()
                acc[:cut] += jnp.dot(rx[d - 1, k, :cut], w_part(k), preferred_element_type=f32)
            y = acc[:cut].astype(bf)
            finish(d, y, 0, range(S - 1), last)
            fronts = y
        for k in range(split, NC - 1):
            by_block(lambda count: x_part(d, k, 1, count).wait_recv())
            acc[cut:] += jnp.dot(rx[d - 1, k, cut:], w_part(k), preferred_element_type=f32)
        by_block(lambda count: x_part(d, NC - 1, 1, count).wait_recv())
        y = (acc[cut:] + jnp.dot(rx[d - 1, NC - 1, cut:], w_part(NC - 1), preferred_element_type=f32)).astype(bf)

        for j in slots:

            @pl.when(helps(j, c))
            def _(d=d, y=y, j=j):
                for g in range(CORES):
                    for v in range(2):
                        lent_tx[d - 1, g, j, v] = y[L + j * E : L + (j + 1) * E, (2 * v + g) * C : (2 * v + g + 1) * C]
                    give_back(d, g, j).start()

        finish(d, y, cut, [S - 1], last)
        if not last:
            if cut:
                deliver(d, fronts, 0, range(S - 1))
            deliver(d, y, cut, [S - 1])
            send_partner(d, range(S))

    def z_target(i):
        return jnp.where(2 * z >= Z, i, Z - 1 - i)

    def z_copy(i, other):
        to = z_target(i)
        return pltpu.make_async_remote_copy(
            stats_tx.at[other], stats_rx.at[other, z], sz_sem.at[other], rz_sem.at[other],
            device_id={"sp": to, "tp": partner if other else tp}, device_id_type=MESH,
        )

    for i in range(Z):
        for first_core in range(CORES):

            @pl.when(c == first_core)
            def _(i=i, first_core=first_core):
                for core in range(CORES):
                    if core == first_core:
                        pl.when(z_target(i) != z)(z_copy(i, 0).start)
                    else:
                        z_copy(i, 1).start()

    if X > 1:
        if cut:
            deliver(X - 1, fronts, 0, range(S - 1))
        deliver(X - 1, y, cut, [S - 1])
        send_partner(X - 1, range(S))
    for d in range(1, X):
        inv_copy(d).wait_send()
        pl.when(jnp.logical_not(pauses))(x_sent(d, 0, RAW, 0).wait_send)
        pl.when(jnp.logical_not(pauses))(lambda: by_block(lambda count: x_sent(d, RAW, LEAD, 1, count).wait_send()))
        by_block(lambda count: x_sent(d, LEAD, NC, 2, count).wait_send())

        for j in slots:

            @pl.when(helps(j, c))
            def _(d=d, j=j):
                forward(d, j).wait_send()
                for g in range(CORES):
                    give_back(d, g, j).wait_send()

    for j in slots:
        pl.when(lends(j, c))(lend(j).wait_send)
    both_weights.wait_send()
    shares[2].wait_send()
    shares[3].wait_send()
    halves = pltpu.make_async_remote_copy(ybuf, ybuf, sy_sem, ry_sem, device_id={"tp": partner}, device_id_type=MESH)
    halves.wait_send()
    halves.wait_recv()

    def z_whole(other):
        part = stats_rx.at[other, pl.ds(0, Z - 1 + other)]
        return pltpu.make_async_remote_copy(
            part, part, sz_sem.at[other], rz_sem.at[other],
            device_id={"tp": partner if other else tp}, device_id_type=MESH,
        )

    for other in range(CORES):
        if Z - 1 + other:
            z_whole(other).wait_recv()

    for j in slots:
        for g in range(CORES):
            core = CORES - 1 - c if g else c

            @pl.when(lends(j, core))
            def _(g=g, j=j, core=core):
                for d in range(1, X):
                    give_back(d, g, j).wait_recv()
                    at = pl.ds(pl.multiple_of(((x + X - d) % X * CORES + core) * L + L - E, E), E)
                    kbuf[S - 1, at, :] = lent_rx[d - 1, g, 0]
                    vbuf[S - 1, at, :] = lent_rx[d - 1, g, 1]

    entries = [(i, other) for i in range(Z) for other in range(CORES)]
    tops = [stats_rx[other, i, 0] for i, other in entries]
    most = functools.reduce(jnp.maximum, tops)
    factors = [jnp.exp(top - most) for top in tops]
    total = functools.reduce(jnp.add, [f * stats_rx[other, i, 1] for f, (i, other) in zip(factors, entries)])
    weighted = functools.reduce(jnp.add, [f * stats_rx[other, i, 2] for f, (i, other) in zip(factors, entries)])
    ro_ref[...] = (weighted / total).astype(ro_ref.dtype)
    for other in range(CORES):
        if Z - 1 + other:
            z_whole(other).wait_send()


def scoped(dims, semaphores, *refs):
    pl.run_scoped(lambda *held: kernel(dims, *refs, *held), *semaphores)


def write_out(*refs):
    sems = refs[-1]
    count = (len(refs) - 1) // 2
    copies = [pltpu.make_async_copy(refs[i], refs[count + i], sems.at[i]) for i in range(count)]
    for copy in copies:
        copy.start()
    for copy in copies:
        copy.wait()


def body(
    tokens, norm_gain, key_weight, value_weight, cum_gates, new_query, new_key, new_value, new_gate
):
    S, L, D = tokens.shape
    C = key_weight.shape[1]
    H = C // HD
    T = lax.axis_size("tp")
    Z = lax.axis_size("sp")
    X = T // CORES
    BL = T * L
    R = 32 if L % 32 == 0 else L
    KC = 256 if D % 256 == 0 else D // 2
    NC = D // KC
    bf, f32 = jnp.bfloat16, jnp.float32
    hbm = pl.BlockSpec(memory_space=pltpu.HBM)
    dma = pltpu.SemaphoreType.DMA
    regular = pltpu.SemaphoreType.REGULAR
    far = max(X - 1, 1)
    vmem = pl.BlockSpec(memory_space=pltpu.VMEM)
    semaphores = [
        dma((S * L // R,)), dma, dma, dma((4,)), regular((max(Z - 2, 1),)), regular, regular,
        dma((far, 3)), dma((far, NC + TAIL)), dma((far,)), dma((far,)), dma((3,)), dma((3,)),
        dma, dma, dma((CORES,)), dma((CORES,)),
        dma((SLOTS,)), dma((SLOTS,)), dma((far, SLOTS)), dma((far, SLOTS)),
        *(dma((far, CORES, SLOTS)) for _ in range(4)),
    ]
    results = pl.pallas_call(
        functools.partial(scoped, (S, L, R, T, Z), semaphores),
        out_shape=(
            pltpu.VMEM((S, BL, C), bf),
            pltpu.VMEM((S, BL, C), bf),
            pltpu.VMEM((S, C), bf),
        ),
        in_specs=[hbm] * 9,
        out_specs=(vmem, vmem, vmem),
        scratch_shapes=[
            pltpu.VMEM((S * L, D), bf),
            pltpu.VMEM((RAW, S * L, KC), bf),
            pltpu.VMEM((S * L, KC), f32),
            pltpu.VMEM((NC, S * L, KC), bf),
            pltpu.VMEM((far, NC, S * L + SLOTS * EXTRA, KC), bf),
            pltpu.VMEM((S * L + SLOTS * EXTRA, 4 * C), f32),
            pltpu.VMEM((D, 4 * C), bf),
            pltpu.VMEM((X, 2, S * L, C), bf),
            pltpu.VMEM((D // 128, 128), bf),
            pltpu.VMEM((1, D), f32),
            pltpu.VMEM((CORES, S, H, BL), f32),
            pltpu.VMEM((4, S, C), bf),
            pltpu.VMEM((S, H), f32),
            pltpu.VMEM((1, S * L), f32),
            pltpu.VMEM((far, 1, S * L), f32),
            pltpu.VMEM((S, CORES, C, C), bf),
            pltpu.VMEM((X, S, CORES, L + SLOTS * EXTRA, C), f32),
            pltpu.VMEM((CORES, 3, S, C), f32),
            pltpu.VMEM((CORES, Z, 3, S, C), f32),
            pltpu.VMEM((SLOTS, NC, EXTRA, KC), bf),
            pltpu.VMEM((far, CORES, SLOTS, 2, EXTRA, C), bf),
            pltpu.VMEM((far, CORES, 2, EXTRA, C), bf),
        ],
        compiler_params=pltpu.CompilerParams(
            collective_id=0, has_side_effects=True, vmem_limit_bytes=56 * 1024 * 1024
        ),
    )(
        tokens.reshape(S * L, D),
        norm_gain.reshape(D // 128, 128),
        key_weight,
        value_weight,
        jnp.transpose(cum_gates, (0, 2, 1)),
        new_query,
        new_key,
        new_value,
        new_gate,
    )
    return pl.pallas_call(
        write_out,
        out_shape=tuple(jax.ShapeDtypeStruct(r.shape, r.dtype) for r in results),
        in_specs=[vmem] * 3,
        out_specs=(hbm, hbm, hbm),
        scratch_shapes=[dma((3,))],
    )(*(pltpu.with_memory_space_constraint(r, pltpu.VMEM) for r in results))


def solution(mesh):
    in_specs = (
        P("gr", ("sp", "tp"), None),
        P(),
        P(None, "tp"),
        P(None, "tp"),
        P("gr", "sp", "tp"),
        P("gr", "tp"),
        P("gr", "tp"),
        P("gr", "tp"),
        P("gr", "tp"),
    )
    out_specs = (P("gr", "sp", "tp"), P("gr", "sp", "tp"), P("gr", "tp"))
    return jax.shard_map(body, mesh=mesh, in_specs=in_specs, out_specs=out_specs, check_vma=False)
```

```python
import functools

import jax
import jax.numpy as jnp
from jax import lax
from jax.experimental import pallas as pl
from jax.experimental.pallas import tpu as pltpu
from jax.sharding import PartitionSpec as P

HD = 64
CORES = 2
LEAD = 4
TAIL = 4
EXTRA, SLOTS = 8, 2
RAW = 2

epsilon = 1e-06
masked_score = -1e30
MESH = pl.DeviceIdType.MESH


def kernel(
    dims,
    tok_hbm, gain_hbm, wk_hbm, wv_hbm, gates_hbm, q_hbm, nk_hbm, nv_hbm, ng_hbm,
    kbuf, vbuf, ro_ref,
    tok, raw, inv, nb, rx, acc, wbuf, ybuf, gain_v, gain_row, gates_v, new_v, ng_v,
    inv_tx, inv_rx, qblock, gate_rep, stats_tx, stats_rx, lent, lent_tx, lent_rx,
    loc_sem, raw_sem, w_sem, small_sem, hop_sem, answer_sem, ready_sem,
    sx_sem, rx_sem, si_sem, ri_sem, sw_sem, rw_sem, sy_sem, ry_sem, sz_sem, rz_sem,
    sl_sem, rl_sem, sf_sem, rf_sem, sg_sem, rg_sem, sk_sem, rk_sem,
):
    S, L, R, T, Z = dims
    X = T // CORES
    f32, bf = jnp.float32, jnp.bfloat16
    rows_each, D = tok.shape
    NC, KC = nb.shape[0], nb.shape[2]
    blocks = rows_each // R
    C = kbuf.shape[2]
    H = C // HD
    BL = T * L
    E, EE = EXTRA, SLOTS * EXTRA
    kept = rows_each - 2 * E
    tp = lax.axis_index("tp")
    z = lax.axis_index("sp")
    x, c = tp // CORES, tp % CORES
    loans = [(Z - 1, 0, 0, 0, E), (Z - 2, 0, 1, 1, E), (Z - 1, 1, 1, 1, 2 * E)][: 3 if Z > 3 else min(Z - 1, 2)]
    slots = range(len(loans))

    def lends(j, core):
        return jnp.logical_and(z == loans[j][0], core >= loans[j][2])

    def helps(j, core):
        return jnp.logical_and(z == loans[j][1], core >= loans[j][2])

    lent_rows = sum((lends(j, c).astype(jnp.int32) for j in slots), 0 * z)
    pauses = c != 0
    partner = x * CORES + (CORES - 1 - c)

    def peer(d):
        return {"tp": ((x + d) % X) * CORES + c}

    def rows(j):
        return pl.ds(j * R, R)

    first = [pltpu.make_async_copy(tok_hbm.at[:, pl.ds(k * KC, KC)], raw.at[k], raw_sem.at[k]) for k in range(RAW)]
    for copy in first:
        copy.start()
    rx[:, :, kept:, :] = jnp.zeros((rx.shape[0], NC, 2 * E + EE, KC), bf)
    barrier = pltpu.get_barrier_semaphore()
    for d in range(1, X):
        pl.semaphore_signal(barrier, inc=1, device_id=peer(d), device_id_type=MESH)
    sides = (z > 0).astype(jnp.int32) + (z < Z - 1).astype(jnp.int32)

    def greet_sides(sem):
        @pl.when(z > 0)
        def _():
            pl.semaphore_signal(sem, inc=1, device_id={"sp": z - 1}, device_id_type=MESH)

        @pl.when(z < Z - 1)
        def _():
            pl.semaphore_signal(sem, inc=1, device_id={"sp": z + 1}, device_id_type=MESH)

    @pl.when(z < Z - 1)
    def _():
        pl.semaphore_signal(barrier, inc=1, device_id={"sp": z + 1}, device_id_type=MESH)

    pl.semaphore_signal(barrier, inc=1, device_id={"tp": partner}, device_id_type=MESH)

    loads = [pltpu.make_async_copy(tok_hbm.at[rows(j)], tok.at[rows(j)], loc_sem.at[j]) for j in range(blocks)]
    small = [
        pltpu.make_async_copy(src, dst, small_sem.at[min(i, 3)])
        for i, (src, dst) in enumerate(
            [(gain_hbm, gain_v), (gates_hbm, gates_v.at[0]), (ng_hbm, ng_v), (q_hbm, new_v.at[0]), (nk_hbm, new_v.at[1]), (nv_hbm, new_v.at[2])]
        )
    ]
    for copy in loads:
        copy.start()
    for copy in small:
        copy.start()
    w_copies = [
        pltpu.make_async_copy(src, wbuf.at[:, pl.ds(2 * i * C, C)], w_sem) for i, src in enumerate((wk_hbm, wv_hbm))
    ]

    def to_partner(src, dst, i):
        return pltpu.make_async_remote_copy(
            src, dst, sw_sem.at[i], rw_sem.at[i], device_id={"tp": partner}, device_id_type=MESH
        )

    shares = [
        to_partner(wk_hbm, wbuf.at[:, pl.ds(C, C)], 0),
        to_partner(wv_hbm, wbuf.at[:, pl.ds(3 * C, C)], 0),
        to_partner(gates_hbm, gates_v.at[1], 1),
        to_partner(q_hbm, new_v.at[3], 2),
    ]
    both_weights = to_partner(wbuf.at[:, pl.ds(0, 2 * C)], wbuf.at[:, pl.ds(0, 2 * C)], 0)

    HALF = NC // 2

    def x_copy(d, k, count=rows_each):
        return pltpu.make_async_remote_copy(
            raw.at[k] if k < RAW else nb.at[k, pl.ds(0, count)],
            rx.at[d - 1, k, pl.ds(0, count)],
            sx_sem.at[d - 1, (k >= RAW) + (k >= LEAD)],
            rx_sem.at[d - 1, k],
            device_id=peer(d),
            device_id_type=MESH,
        )

    def x_sent(d, first, stop, group, count=rows_each):
        part = rx.at[d - 1, pl.ds(first, stop - first), pl.ds(0, count)]
        return pltpu.make_async_remote_copy(
            part, part, sx_sem.at[d - 1, group], rx_sem.at[d - 1, 0], device_id=peer(d), device_id_type=MESH
        )

    cut, split = (S - 1) * L, NC - TAIL

    def x_part(d, k, part, count=rows_each):
        at = pl.ds(cut, count - cut) if part else pl.ds(0, cut)
        return pltpu.make_async_remote_copy(
            nb.at[k, at], rx.at[d - 1, k, at], sx_sem.at[d - 1, 2], rx_sem.at[d - 1, k + TAIL * part],
            device_id=peer(d), device_id_type=MESH,
        )

    def x_arrival(d, k, count=rows_each):
        part = rx.at[d - 1, k, pl.ds(0, count)]
        return pltpu.make_async_remote_copy(
            part, part, sx_sem.at[d - 1, 0], rx_sem.at[d - 1, k], device_id=peer(d), device_id_type=MESH
        )

    def by_block(act):
        for i in range(3):
            pl.when(lent_rows == i)(lambda: act(rows_each - i * E))

    def to_block(src, dst, send_sem, recv_sem, block, target):
        return pltpu.make_async_remote_copy(
            src, dst, send_sem, recv_sem, device_id={"sp": block, "tp": target}, device_id_type=MESH
        )

    def lend(j):
        _, block, _, slot, back = loans[j]
        return to_block(nb.at[:, pl.ds(rows_each - back, E)], lent.at[slot], sl_sem.at[j], rl_sem.at[j], block, tp)

    def forward(d, j):
        slot = loans[j][3]
        return pltpu.make_async_remote_copy(
            lent.at[slot], rx.at[d - 1, :, pl.ds(rows_each + slot * E, E)], sf_sem.at[d - 1, j], rf_sem.at[d - 1, j],
            device_id=peer(d), device_id_type=MESH,
        )

    def gate_copy(d, g, j):
        _, block, _, slot, back = loans[j]
        return to_block(
            gate_rep.at[d, S - 1, g, pl.ds(L - back, E)], gate_rep.at[d, S - 1, g, pl.ds(L + slot * E, E)],
            sg_sem.at[d - 1, g, j], rg_sem.at[d - 1, g, j], block, tp,
        )

    def give_back(d, g, j):
        return to_block(
            lent_tx.at[d - 1, g, loans[j][3]], lent_rx.at[d - 1, g, j], sk_sem.at[d - 1, g, j], rk_sem.at[d - 1, g, j],
            loans[j][0], partner if g else tp,
        )

    def inv_copy(d):
        return pltpu.make_async_remote_copy(
            inv_tx, inv_rx.at[d - 1], si_sem.at[d - 1], ri_sem.at[d - 1], device_id=peer(d), device_id_type=MESH
        )

    def norm(v, r, k):
        return (v.astype(f32) * r * gain_row[:, pl.ds(k * KC, KC)]).astype(bf)

    before = (z > 0).astype(jnp.int32)
    pl.semaphore_wait(barrier, 1 + (X - 1) + before)

    def send(chunks, count=rows_each):
        for k in chunks:
            for d in range(1, X):
                x_copy(d, k, count).start()

    for k in range(RAW):
        first[k].wait()
        send([k])

    @pl.when(z > 0)
    def _():
        pl.semaphore_signal(answer_sem, inc=1, device_id={"sp": z - 1}, device_id_type=MESH)


    small[0].wait()
    g = gain_v[...].astype(f32)
    lanes = g.shape[1]
    for i in range(g.shape[0]):
        gain_row[:, pl.ds(i * lanes, lanes)] = g[i : i + 1, :]
    for j in range(blocks):
        loads[j].wait()
        v = tok[rows(j), :].astype(f32)
        r = lax.rsqrt(jnp.mean(v * v, axis=-1, keepdims=True) + epsilon)
        inv[rows(j), :] = jnp.broadcast_to(r, (R, KC))
    for copy in w_copies:
        copy.start()
    eye = lax.broadcasted_iota(jnp.int32, (rows_each, rows_each), 0) == lax.broadcasted_iota(
        jnp.int32, (rows_each, rows_each), 1
    )
    inv_tx[...] = jnp.sum(jnp.where(eye, inv[:, :rows_each], 0.0), axis=0, keepdims=True)
    for k in range(RAW, NC):
        nb[k] = norm(tok[:, pl.ds(k * KC, KC)], inv[...], k)
        if k < LEAD:
            by_block(lambda count: send([k], count))
        if k == RAW:
            for d in range(1, X):
                inv_copy(d).start()
        if k == HALF - 1:
            pl.when(jnp.logical_not(pauses))(lambda: by_block(lambda count: send(range(LEAD, HALF), count)))
    for copy in shares[2:] + shares[:2]:
        copy.start()
    for k in range(RAW):
        nb[k] = norm(raw[k], inv[...], k)
    pl.when(z < Z - 1)(lambda: pl.semaphore_wait(answer_sem, 1))
    for r in range(Z - 2):
        greet_sides(hop_sem.at[r])
        pl.semaphore_wait(hop_sem.at[r], sides)
    for j in slots:
        pl.when(lends(j, c))(lend(j).start)

    @pl.when(pauses)
    def _():
        for d in range(1, X):
            x_sent(d, 0, RAW, 0).wait_send()
            by_block(lambda count: x_sent(d, RAW, LEAD, 1, count).wait_send())

    small[1].wait()
    small[2].wait()
    pltpu.make_async_copy(new_v.at[pl.ds(0, 3)], new_v.at[pl.ds(0, 3)], small_sem.at[3]).wait()
    for i in (2, 3):
        shares[i].wait_recv()

    scale = HD ** (-0.5)
    lane_head = lax.broadcasted_iota(jnp.int32, (C, C), 1) // HD
    same_head = lane_head == lax.broadcasted_iota(jnp.int32, (C, C), 0) // HD
    diagonal = lax.broadcasted_iota(jnp.int32, (C, C), 0) == lax.broadcasted_iota(jnp.int32, (C, C), 1)
    own_head = lax.broadcasted_iota(jnp.int32, (H, C), 1) // HD == lax.broadcasted_iota(jnp.int32, (H, C), 0)
    heads_eye = lax.broadcasted_iota(jnp.int32, (H, H), 0) == lax.broadcasted_iota(jnp.int32, (H, H), 1)
    last_block = z == Z - 1

    def as_row(column):
        return jnp.sum(jnp.where(own_head, column, 0.0), axis=0, keepdims=True)

    def source(d):
        return ((x + X - d) % X) * CORES + c

    for s in range(S):
        for g in range(CORES):
            column = jnp.sum(jnp.where(diagonal, new_v[3 * g, s : s + 1, :].astype(f32), 0.0), axis=1, keepdims=True)
            qblock[s, g] = jnp.where(same_head, column, 0.0).astype(bf)
    head_of_lane = lax.broadcasted_iota(jnp.int32, (L, C), 1) // HD
    for d in range(X):
        pick = lax.broadcasted_iota(jnp.int32, (L, BL), 1) == lax.broadcasted_iota(
            jnp.int32, (L, BL), 0
        ) + source(d) * L
        for s in range(S):
            for g in range(CORES):
                spread = jnp.zeros((L, C), f32)
                for h in range(H):
                    column = jnp.sum(jnp.where(pick, gates_v[g, s, h : h + 1, :], 0.0), axis=1, keepdims=True)
                    spread = jnp.where(head_of_lane == h, column, spread)
                gate_rep[d, s, g, :L] = spread

                for slot in range(SLOTS):
                    theirs = functools.reduce(jnp.logical_or, [helps(j, c) for j in slots if loans[j][3] == slot], z < 0)

                    @pl.when(jnp.logical_not(theirs))
                    def _(d=d, s=s, g=g, slot=slot):
                        gate_rep[d, s, g, L + slot * E : L + (slot + 1) * E] = jnp.full((E, C), -masked_score, f32)

    for s in range(S):
        fresh = jnp.dot(new_v[1, s : s + 1, :], qblock[s, 0], preferred_element_type=f32) * scale
        own_gate = jnp.sum(jnp.where(heads_eye, ng_v[s : s + 1, :], 0.0), axis=1, keepdims=True)
        fresh = jnp.where(last_block, fresh - as_row(gates_v[0, s, :, BL - 1 : BL] + own_gate), masked_score)
        weight = jnp.where(last_block, jnp.ones_like(fresh), 0.0)
        stats_tx[0, 0, s : s + 1, :] = fresh
        stats_tx[0, 1, s : s + 1, :] = weight
        stats_tx[0, 2, s : s + 1, :] = weight * new_v[2, s : s + 1, :].astype(f32)
        stats_tx[1, 0, s : s + 1, :] = jnp.full((1, C), masked_score, f32)
        stats_tx[1, 1, s : s + 1, :] = jnp.zeros((1, C), f32)
        stats_tx[1, 2, s : s + 1, :] = jnp.zeros((1, C), f32)

    pl.when(pauses)(lambda: by_block(lambda count: send(range(LEAD, HALF), count)))
    for d in range(1, X):
        for g in range(CORES):
            for j in slots:
                pl.when(lends(j, c))(gate_copy(d, g, j).start)
    for d in range(1, X):
        inv_copy(d).wait_recv()
        r = jnp.sum(jnp.where(eye, inv_rx[d - 1], 0.0), axis=1, keepdims=True)
        for k in range(RAW):
            x_arrival(d, k).wait_recv()
            rx[d - 1, k, :rows_each] = norm(rx[d - 1, k, :rows_each], r, k)

    def w_part(k):
        return wbuf[pl.ds(k * KC if isinstance(k, int) else pl.multiple_of(k * KC, KC), KC), :]

    def y_copy(d, s, v):
        at = pl.ds(pl.multiple_of(source(d) * L, L), L)
        return pltpu.make_async_remote_copy(
            ybuf.at[d, v, pl.ds(s * L, L)], (kbuf, vbuf)[v].at[s, at],
            sy_sem, ry_sem, device_id={"tp": partner}, device_id_type=MESH,
        )

    def rows_of(d, s):
        return L + EE if d and s == S - 1 else L

    def finish(d, y, first, prompts, last):
        pairs = [(g, s) for g in range(CORES) for s in prompts]
        before = {(g, s): [stats_tx[g, i, s : s + 1, :] for i in range(3)] for g, s in pairs}
        scores = {}
        for g, s in pairs:
            count = rows_of(d, s)
            keys = y[s * L - first : s * L - first + count, g * C : (g + 1) * C]
            scores[g, s] = jnp.dot(keys, qblock[s, g], preferred_element_type=f32) * scale - gate_rep[d, s, g, :count]
        after = {}
        for g, s in pairs:
            old_top, old_total, old_weighted = before[g, s]
            values = y[s * L - first : s * L - first + rows_of(d, s), (2 + g) * C : (3 + g) * C].astype(f32)
            top = jnp.maximum(jnp.max(scores[g, s], axis=0, keepdims=True), old_top)
            weights = jnp.exp(scores[g, s] - top)
            factor = jnp.exp(old_top - top)
            total = jnp.sum(weights, axis=0, keepdims=True) + factor * old_total
            weighted = jnp.sum(weights * values, axis=0, keepdims=True) + factor * old_weighted
            after[g, s] = (top, total, weighted)
        for g, s in pairs:
            for i, row in enumerate(after[g, s]):
                stats_tx[g, i, s : s + 1, :] = row
        if last:
            for s in prompts:
                for i, row in enumerate(after[0, s]):
                    stats_rx[0, z, i, s : s + 1, :] = row

    def deliver(d, y, first, prompts):
        place = pl.ds(pl.multiple_of(source(d) * L, L), L)
        for s in prompts:
            part = y[s * L - first : (s + 1) * L - first]
            kbuf[s, place, :] = part[:, :C]
            vbuf[s, place, :] = part[:, 2 * C : 3 * C]
            ybuf[d, 0, s * L : (s + 1) * L] = part[:, C : 2 * C]
            ybuf[d, 1, s * L : (s + 1) * L] = part[:, 3 * C :]

    def send_partner(d, prompts):
        for s in prompts:
            for v in range(2):
                y_copy(d, s, v).start()

    pltpu.make_async_copy(wbuf.at[:, pl.ds(0, 2 * C)], wbuf.at[:, pl.ds(0, 2 * C)], w_sem).wait()
    both_weights.wait_recv()

    for j in slots:

        @pl.when(helps(j, c))
        def _(j=j):
            lend(j).wait_recv()
            for d in range(1, X):
                forward(d, j).start()

    by_block(lambda count: send(range(HALF, split), count))
    for part in range(2):
        for k in range(split, NC):
            for d in range(1, X):
                by_block(lambda count: x_part(d, k, part, count).start())
    acc[...] = jnp.zeros_like(acc)

    def near(k, carry):
        acc[:rows_each] += jnp.dot(nb[k], w_part(k), preferred_element_type=f32)
        return carry

    lax.fori_loop(0, NC, near, 0)
    y = acc[:rows_each].astype(bf)
    deliver(0, y, 0, range(S))
    finish(0, y, 0, range(S), X == 1)
    send_partner(0, range(S))
    pl.semaphore_signal(ready_sem, inc=1, device_id={"tp": partner}, device_id_type=MESH)
    for d in range(1, X):
        for g in range(CORES):

            for j in slots:

                @pl.when(lends(j, c))
                def _(d=d, g=g, j=j):
                    gate_copy(d, g, j).wait_send()
                    back = L - loans[j][4]
                    gate_rep[d, S - 1, g, back : back + E] = jnp.full((E, C), -masked_score, f32)

                pl.when(helps(j, c))(gate_copy(d, g, j).wait_recv)
    pl.semaphore_wait(ready_sem, 1)

    for d in range(1, X):
        acc[...] = jnp.zeros_like(acc)

        def far(k, carry, d=d):
            acc[...] += jnp.dot(rx[d - 1, k], w_part(k), preferred_element_type=f32)
            return carry

        def far_arriving(k, carry, d=d):
            by_block(lambda count: x_arrival(d, k, count).wait_recv())
            return far(k, carry, d)

        for j in slots:
            pl.when(helps(j, c))(forward(d, j).wait_recv)
        lax.fori_loop(0, RAW, far, 0)
        lax.fori_loop(RAW, split, far_arriving, 0)
        last = d == X - 1
        if cut:
            for k in range(split, NC):
                x_part(d, k, 0).wait_recv()
                acc[:cut] += jnp.dot(rx[d - 1, k, :cut], w_part(k), preferred_element_type=f32)
            y = acc[:cut].astype(bf)
            finish(d, y, 0, range(S - 1), last)
            fronts = y
        for k in range(split, NC - 1):
            by_block(lambda count: x_part(d, k, 1, count).wait_recv())
            acc[cut:] += jnp.dot(rx[d - 1, k, cut:], w_part(k), preferred_element_type=f32)
        by_block(lambda count: x_part(d, NC - 1, 1, count).wait_recv())
        y = (acc[cut:] + jnp.dot(rx[d - 1, NC - 1, cut:], w_part(NC - 1), preferred_element_type=f32)).astype(bf)

        for j in slots:

            @pl.when(helps(j, c))
            def _(d=d, y=y, j=j):
                for g in range(CORES):
                    for v in range(2):
                        slot = loans[j][3]
                        rows_back = y[L + slot * E : L + (slot + 1) * E]
                        lent_tx[d - 1, g, slot, v] = rows_back[:, (2 * v + g) * C : (2 * v + g + 1) * C]
                    give_back(d, g, j).start()

        finish(d, y, cut, [S - 1], last)
        if not last:
            if cut:
                deliver(d, fronts, 0, range(S - 1))
            deliver(d, y, cut, [S - 1])
            send_partner(d, range(S))

    def z_target(i):
        return jnp.where(2 * z >= Z, i, Z - 1 - i)

    def z_copy(i, other):
        to = z_target(i)
        return pltpu.make_async_remote_copy(
            stats_tx.at[other], stats_rx.at[other, z], sz_sem.at[other], rz_sem.at[other],
            device_id={"sp": to, "tp": partner if other else tp}, device_id_type=MESH,
        )

    for i in range(Z):
        for first_core in range(CORES):

            @pl.when(c == first_core)
            def _(i=i, first_core=first_core):
                for core in range(CORES):
                    if core == first_core:
                        pl.when(z_target(i) != z)(z_copy(i, 0).start)
                    else:
                        z_copy(i, 1).start()

    if X > 1:
        if cut:
            deliver(X - 1, fronts, 0, range(S - 1))
        deliver(X - 1, y, cut, [S - 1])
        send_partner(X - 1, range(S))
    for d in range(1, X):
        inv_copy(d).wait_send()
        pl.when(jnp.logical_not(pauses))(x_sent(d, 0, RAW, 0).wait_send)
        pl.when(jnp.logical_not(pauses))(lambda: by_block(lambda count: x_sent(d, RAW, LEAD, 1, count).wait_send()))
        by_block(lambda count: x_sent(d, LEAD, NC, 2, count).wait_send())

        for j in slots:

            @pl.when(helps(j, c))
            def _(d=d, j=j):
                forward(d, j).wait_send()
                for g in range(CORES):
                    give_back(d, g, j).wait_send()

    for j in slots:
        pl.when(lends(j, c))(lend(j).wait_send)
    both_weights.wait_send()
    shares[2].wait_send()
    shares[3].wait_send()
    halves = pltpu.make_async_remote_copy(ybuf, ybuf, sy_sem, ry_sem, device_id={"tp": partner}, device_id_type=MESH)
    halves.wait_send()
    halves.wait_recv()

    def z_whole(other):
        part = stats_rx.at[other, pl.ds(0, Z - 1 + other)]
        return pltpu.make_async_remote_copy(
            part, part, sz_sem.at[other], rz_sem.at[other],
            device_id={"tp": partner if other else tp}, device_id_type=MESH,
        )

    for other in range(CORES):
        if Z - 1 + other:
            z_whole(other).wait_recv()

    for j in slots:
        for g in range(CORES):
            core = CORES - 1 - c if g else c

            @pl.when(lends(j, core))
            def _(g=g, j=j, core=core):
                for d in range(1, X):
                    give_back(d, g, j).wait_recv()
                    at = pl.ds(pl.multiple_of(((x + X - d) % X * CORES + core) * L + L - loans[j][4], E), E)
                    kbuf[S - 1, at, :] = lent_rx[d - 1, g, j, 0]
                    vbuf[S - 1, at, :] = lent_rx[d - 1, g, j, 1]

    entries = [(i, other) for i in range(Z) for other in range(CORES)]
    tops = [stats_rx[other, i, 0] for i, other in entries]
    most = functools.reduce(jnp.maximum, tops)
    factors = [jnp.exp(top - most) for top in tops]
    total = functools.reduce(jnp.add, [f * stats_rx[other, i, 1] for f, (i, other) in zip(factors, entries)])
    weighted = functools.reduce(jnp.add, [f * stats_rx[other, i, 2] for f, (i, other) in zip(factors, entries)])
    ro_ref[...] = (weighted / total).astype(ro_ref.dtype)
    for other in range(CORES):
        if Z - 1 + other:
            z_whole(other).wait_send()


def scoped(dims, semaphores, *refs):
    pl.run_scoped(lambda *held: kernel(dims, *refs, *held), *semaphores)


def write_out(*refs):
    sems = refs[-1]
    count = (len(refs) - 1) // 2
    copies = [pltpu.make_async_copy(refs[i], refs[count + i], sems.at[i]) for i in range(count)]
    for copy in copies:
        copy.start()
    for copy in copies:
        copy.wait()


def body(
    tokens, norm_gain, key_weight, value_weight, cum_gates, new_query, new_key, new_value, new_gate
):
    S, L, D = tokens.shape
    C = key_weight.shape[1]
    H = C // HD
    T = lax.axis_size("tp")
    Z = lax.axis_size("sp")
    X = T // CORES
    BL = T * L
    R = 32 if L % 32 == 0 else L
    KC = 256 if D % 256 == 0 else D // 2
    NC = D // KC
    bf, f32 = jnp.bfloat16, jnp.float32
    hbm = pl.BlockSpec(memory_space=pltpu.HBM)
    dma = pltpu.SemaphoreType.DMA
    regular = pltpu.SemaphoreType.REGULAR
    far = max(X - 1, 1)
    vmem = pl.BlockSpec(memory_space=pltpu.VMEM)
    semaphores = [
        dma((S * L // R,)), dma((RAW,)), dma, dma((4,)), regular((max(Z - 2, 1),)), regular, regular,
        dma((far, 3)), dma((far, NC + TAIL)), dma((far,)), dma((far,)), dma((3,)), dma((3,)),
        dma, dma, dma((CORES,)), dma((CORES,)),
        dma((3,)), dma((3,)), dma((far, 3)), dma((far, 3)),
        *(dma((far, CORES, 3)) for _ in range(4)),
    ]
    results = pl.pallas_call(
        functools.partial(scoped, (S, L, R, T, Z), semaphores),
        out_shape=(
            pltpu.VMEM((S, BL, C), bf),
            pltpu.VMEM((S, BL, C), bf),
            pltpu.VMEM((S, C), bf),
        ),
        in_specs=[hbm] * 9,
        out_specs=(vmem, vmem, vmem),
        scratch_shapes=[
            pltpu.VMEM((S * L, D), bf),
            pltpu.VMEM((RAW, S * L, KC), bf),
            pltpu.VMEM((S * L, KC), f32),
            pltpu.VMEM((NC, S * L, KC), bf),
            pltpu.VMEM((far, NC, S * L + SLOTS * EXTRA, KC), bf),
            pltpu.VMEM((S * L + SLOTS * EXTRA, 4 * C), f32),
            pltpu.VMEM((D, 4 * C), bf),
            pltpu.VMEM((X, 2, S * L, C), bf),
            pltpu.VMEM((D // 128, 128), bf),
            pltpu.VMEM((1, D), f32),
            pltpu.VMEM((CORES, S, H, BL), f32),
            pltpu.VMEM((4, S, C), bf),
            pltpu.VMEM((S, H), f32),
            pltpu.VMEM((1, S * L), f32),
            pltpu.VMEM((far, 1, S * L), f32),
            pltpu.VMEM((S, CORES, C, C), bf),
            pltpu.VMEM((X, S, CORES, L + SLOTS * EXTRA, C), f32),
            pltpu.VMEM((CORES, 3, S, C), f32),
            pltpu.VMEM((CORES, Z, 3, S, C), f32),
            pltpu.VMEM((SLOTS, NC, EXTRA, KC), bf),
            pltpu.VMEM((far, CORES, SLOTS, 2, EXTRA, C), bf),
            pltpu.VMEM((far, CORES, 3, 2, EXTRA, C), bf),
        ],
        compiler_params=pltpu.CompilerParams(
            collective_id=0, has_side_effects=True, vmem_limit_bytes=56 * 1024 * 1024
        ),
    )(
        tokens.reshape(S * L, D),
        norm_gain.reshape(D // 128, 128),
        key_weight,
        value_weight,
        jnp.transpose(cum_gates, (0, 2, 1)),
        new_query,
        new_key,
        new_value,
        new_gate,
    )
    return pl.pallas_call(
        write_out,
        out_shape=tuple(jax.ShapeDtypeStruct(r.shape, r.dtype) for r in results),
        in_specs=[vmem] * 3,
        out_specs=(hbm, hbm, hbm),
        scratch_shapes=[dma((3,))],
    )(*(pltpu.with_memory_space_constraint(r, pltpu.VMEM) for r in results))


def solution(mesh):
    in_specs = (
        P("gr", ("sp", "tp"), None),
        P(),
        P(None, "tp"),
        P(None, "tp"),
        P("gr", "sp", "tp"),
        P("gr", "tp"),
        P("gr", "tp"),
        P("gr", "tp"),
        P("gr", "tp"),
    )
    out_specs = (P("gr", "sp", "tp"), P("gr", "sp", "tp"), P("gr", "tp"))
    return jax.shard_map(body, mesh=mesh, in_specs=in_specs, out_specs=out_specs, check_vma=False)
```

```python
import functools

import jax
import jax.numpy as jnp
from jax import lax
from jax.experimental import pallas as pl
from jax.experimental.pallas import tpu as pltpu
from jax.sharding import PartitionSpec as P

HD = 64
CORES = 2
LEAD = 3
TAIL = 4
EXTRA, SLOTS = 8, 2
RAW = 2

epsilon = 1e-06
masked_score = -1e30
MESH = pl.DeviceIdType.MESH


def kernel(
    dims,
    tok_hbm, gain_hbm, wk_hbm, wv_hbm, gates_hbm, q_hbm, nk_hbm, nv_hbm, ng_hbm,
    kbuf, vbuf, ro_ref,
    tok, raw, inv, nb, rx, acc, wbuf, ybuf, gain_v, gain_row, gates_v, new_v, ng_v,
    inv_tx, inv_rx, qblock, gate_rep, stats_tx, stats_rx, lent, lent_tx, lent_rx,
    loc_sem, raw_sem, w_sem, small_sem, hop_sem, answer_sem, ready_sem,
    sx_sem, rx_sem, si_sem, ri_sem, sw_sem, rw_sem, sy_sem, ry_sem, sz_sem, rz_sem,
    sl_sem, rl_sem, sf_sem, rf_sem, sg_sem, rg_sem, sk_sem, rk_sem,
):
    S, L, R, T, Z = dims
    X = T // CORES
    f32, bf = jnp.float32, jnp.bfloat16
    rows_each, D = tok.shape
    NC, KC = nb.shape[0], nb.shape[2]
    blocks = rows_each // R
    C = kbuf.shape[2]
    H = C // HD
    BL = T * L
    E, EE = EXTRA, SLOTS * EXTRA
    kept = rows_each - 2 * E
    tp = lax.axis_index("tp")
    z = lax.axis_index("sp")
    x, c = tp // CORES, tp % CORES
    loans = [(Z - 1, 0, 0, 0, E), (Z - 2, 0, 1, 1, E), (Z - 1, 1, 1, 1, 2 * E)][: 3 if Z > 3 else min(Z - 1, 2)]
    slots = range(len(loans))

    def lends(j, core):
        return jnp.logical_and(z == loans[j][0], core >= loans[j][2])

    def helps(j, core):
        return jnp.logical_and(z == loans[j][1], core >= loans[j][2])

    lent_rows = sum((lends(j, c).astype(jnp.int32) for j in slots), 0 * z)
    pauses = c != 0
    partner = x * CORES + (CORES - 1 - c)

    def peer(d):
        return {"tp": ((x + d) % X) * CORES + c}

    def rows(j):
        return pl.ds(j * R, R)

    first = [pltpu.make_async_copy(tok_hbm.at[:, pl.ds(k * KC, KC)], raw.at[k], raw_sem.at[k]) for k in range(RAW)]
    for copy in first:
        copy.start()
    rx[:, :, kept:, :] = jnp.zeros((rx.shape[0], NC, 2 * E + EE, KC), bf)
    barrier = pltpu.get_barrier_semaphore()
    for d in range(1, X):
        pl.semaphore_signal(barrier, inc=1, device_id=peer(d), device_id_type=MESH)
    sides = (z > 0).astype(jnp.int32) + (z < Z - 1).astype(jnp.int32)

    def greet_sides(sem):
        @pl.when(z > 0)
        def _():
            pl.semaphore_signal(sem, inc=1, device_id={"sp": z - 1}, device_id_type=MESH)

        @pl.when(z < Z - 1)
        def _():
            pl.semaphore_signal(sem, inc=1, device_id={"sp": z + 1}, device_id_type=MESH)

    @pl.when(z < Z - 1)
    def _():
        pl.semaphore_signal(barrier, inc=1, device_id={"sp": z + 1}, device_id_type=MESH)

    pl.semaphore_signal(barrier, inc=1, device_id={"tp": partner}, device_id_type=MESH)

    loads = [pltpu.make_async_copy(tok_hbm.at[rows(j)], tok.at[rows(j)], loc_sem.at[j]) for j in range(blocks)]
    small = [
        pltpu.make_async_copy(src, dst, small_sem.at[min(i, 3)])
        for i, (src, dst) in enumerate(
            [(gain_hbm, gain_v), (gates_hbm, gates_v.at[0]), (ng_hbm, ng_v), (q_hbm, new_v.at[0]), (nk_hbm, new_v.at[1]), (nv_hbm, new_v.at[2])]
        )
    ]
    for copy in loads:
        copy.start()
    for copy in small:
        copy.start()
    w_copies = [
        pltpu.make_async_copy(src, wbuf.at[:, pl.ds(2 * i * C, C)], w_sem) for i, src in enumerate((wk_hbm, wv_hbm))
    ]

    def to_partner(src, dst, i):
        return pltpu.make_async_remote_copy(
            src, dst, sw_sem.at[i], rw_sem.at[i], device_id={"tp": partner}, device_id_type=MESH
        )

    shares = [
        to_partner(wk_hbm, wbuf.at[:, pl.ds(C, C)], 0),
        to_partner(wv_hbm, wbuf.at[:, pl.ds(3 * C, C)], 0),
        to_partner(gates_hbm, gates_v.at[1], 1),
        to_partner(q_hbm, new_v.at[3], 2),
    ]
    both_weights = to_partner(wbuf.at[:, pl.ds(0, 2 * C)], wbuf.at[:, pl.ds(0, 2 * C)], 0)

    HALF = NC // 2

    def x_copy(d, k, count=rows_each):
        return pltpu.make_async_remote_copy(
            raw.at[k] if k < RAW else nb.at[k, pl.ds(0, count)],
            rx.at[d - 1, k, pl.ds(0, count)],
            sx_sem.at[d - 1, (k >= RAW) + (k >= LEAD)],
            rx_sem.at[d - 1, k],
            device_id=peer(d),
            device_id_type=MESH,
        )

    def x_sent(d, first, stop, group, count=rows_each):
        part = rx.at[d - 1, pl.ds(first, stop - first), pl.ds(0, count)]
        return pltpu.make_async_remote_copy(
            part, part, sx_sem.at[d - 1, group], rx_sem.at[d - 1, 0], device_id=peer(d), device_id_type=MESH
        )

    cut, split = (S - 1) * L, NC - TAIL

    def x_part(d, k, part, count=rows_each):
        at = pl.ds(cut, count - cut) if part else pl.ds(0, cut)
        return pltpu.make_async_remote_copy(
            nb.at[k, at], rx.at[d - 1, k, at], sx_sem.at[d - 1, 2], rx_sem.at[d - 1, k + TAIL * part],
            device_id=peer(d), device_id_type=MESH,
        )

    def x_arrival(d, k, count=rows_each):
        part = rx.at[d - 1, k, pl.ds(0, count)]
        return pltpu.make_async_remote_copy(
            part, part, sx_sem.at[d - 1, 0], rx_sem.at[d - 1, k], device_id=peer(d), device_id_type=MESH
        )

    def by_block(act):
        for i in range(3):
            pl.when(lent_rows == i)(lambda: act(rows_each - i * E))

    def to_block(src, dst, send_sem, recv_sem, block, target):
        return pltpu.make_async_remote_copy(
            src, dst, send_sem, recv_sem, device_id={"sp": block, "tp": target}, device_id_type=MESH
        )

    def lend(j):
        _, block, _, slot, back = loans[j]
        return to_block(nb.at[:, pl.ds(rows_each - back, E)], lent.at[slot], sl_sem.at[j], rl_sem.at[j], block, tp)

    def forward(d, j):
        slot = loans[j][3]
        return pltpu.make_async_remote_copy(
            lent.at[slot], rx.at[d - 1, :, pl.ds(rows_each + slot * E, E)], sf_sem.at[d - 1, j], rf_sem.at[d - 1, j],
            device_id=peer(d), device_id_type=MESH,
        )

    def gate_copy(d, g, j):
        _, block, _, slot, back = loans[j]
        return to_block(
            gate_rep.at[d, S - 1, g, pl.ds(L - back, E)], gate_rep.at[d, S - 1, g, pl.ds(L + slot * E, E)],
            sg_sem.at[d - 1, g, j], rg_sem.at[d - 1, g, j], block, tp,
        )

    def give_back(d, g, j):
        return to_block(
            lent_tx.at[d - 1, g, loans[j][3]], lent_rx.at[d - 1, g, j], sk_sem.at[d - 1, g, j], rk_sem.at[d - 1, g, j],
            loans[j][0], partner if g else tp,
        )

    def inv_copy(d):
        return pltpu.make_async_remote_copy(
            inv_tx, inv_rx.at[d - 1], si_sem.at[d - 1], ri_sem.at[d - 1], device_id=peer(d), device_id_type=MESH
        )

    def norm(v, r, k):
        return (v.astype(f32) * r * gain_row[:, pl.ds(k * KC, KC)]).astype(bf)

    before = (z > 0).astype(jnp.int32)
    pl.semaphore_wait(barrier, 1 + (X - 1) + before)

    def send(chunks, count=rows_each):
        for k in chunks:
            for d in range(1, X):
                x_copy(d, k, count).start()

    for k in range(RAW):
        first[k].wait()
        send([k])

    @pl.when(z > 0)
    def _():
        pl.semaphore_signal(answer_sem, inc=1, device_id={"sp": z - 1}, device_id_type=MESH)


    small[0].wait()
    g = gain_v[...].astype(f32)
    lanes = g.shape[1]
    for i in range(g.shape[0]):
        gain_row[:, pl.ds(i * lanes, lanes)] = g[i : i + 1, :]
    for j in range(blocks):
        loads[j].wait()
        v = tok[rows(j), :].astype(f32)
        r = lax.rsqrt(jnp.mean(v * v, axis=-1, keepdims=True) + epsilon)
        inv[rows(j), :] = jnp.broadcast_to(r, (R, KC))
    for copy in w_copies:
        copy.start()
    eye = lax.broadcasted_iota(jnp.int32, (rows_each, rows_each), 0) == lax.broadcasted_iota(
        jnp.int32, (rows_each, rows_each), 1
    )
    inv_tx[...] = jnp.sum(jnp.where(eye, inv[:, :rows_each], 0.0), axis=0, keepdims=True)
    for k in range(RAW, NC):
        nb[k] = norm(tok[:, pl.ds(k * KC, KC)], inv[...], k)
        if k < LEAD:
            by_block(lambda count: send([k], count))
        if k == RAW:
            for d in range(1, X):
                inv_copy(d).start()
        if k == HALF - 1:
            pl.when(jnp.logical_not(pauses))(lambda: by_block(lambda count: send(range(LEAD, HALF), count)))
    for copy in shares[2:] + shares[:2]:
        copy.start()
    for k in range(RAW):
        nb[k] = norm(raw[k], inv[...], k)
    pl.when(z < Z - 1)(lambda: pl.semaphore_wait(answer_sem, 1))
    for r in range(Z - 2):
        greet_sides(hop_sem.at[r])
        pl.semaphore_wait(hop_sem.at[r], sides)
    for j in slots:
        pl.when(lends(j, c))(lend(j).start)

    @pl.when(pauses)
    def _():
        for d in range(1, X):
            x_sent(d, 0, RAW, 0).wait_send()
            by_block(lambda count: x_sent(d, RAW, LEAD, 1, count).wait_send())

    small[1].wait()
    small[2].wait()
    pltpu.make_async_copy(new_v.at[pl.ds(0, 3)], new_v.at[pl.ds(0, 3)], small_sem.at[3]).wait()
    for i in (2, 3):
        shares[i].wait_recv()

    scale = HD ** (-0.5)
    lane_head = lax.broadcasted_iota(jnp.int32, (C, C), 1) // HD
    same_head = lane_head == lax.broadcasted_iota(jnp.int32, (C, C), 0) // HD
    diagonal = lax.broadcasted_iota(jnp.int32, (C, C), 0) == lax.broadcasted_iota(jnp.int32, (C, C), 1)
    own_head = lax.broadcasted_iota(jnp.int32, (H, C), 1) // HD == lax.broadcasted_iota(jnp.int32, (H, C), 0)
    heads_eye = lax.broadcasted_iota(jnp.int32, (H, H), 0) == lax.broadcasted_iota(jnp.int32, (H, H), 1)
    last_block = z == Z - 1

    def as_row(column):
        return jnp.sum(jnp.where(own_head, column, 0.0), axis=0, keepdims=True)

    def source(d):
        return ((x + X - d) % X) * CORES + c

    for s in range(S):
        for g in range(CORES):
            column = jnp.sum(jnp.where(diagonal, new_v[3 * g, s : s + 1, :].astype(f32), 0.0), axis=1, keepdims=True)
            qblock[s, g] = jnp.where(same_head, column, 0.0).astype(bf)
    head_of_lane = lax.broadcasted_iota(jnp.int32, (L, C), 1) // HD
    for d in range(X):
        pick = lax.broadcasted_iota(jnp.int32, (L, BL), 1) == lax.broadcasted_iota(
            jnp.int32, (L, BL), 0
        ) + source(d) * L
        for s in range(S):
            for g in range(CORES):
                spread = jnp.zeros((L, C), f32)
                for h in range(H):
                    column = jnp.sum(jnp.where(pick, gates_v[g, s, h : h + 1, :], 0.0), axis=1, keepdims=True)
                    spread = jnp.where(head_of_lane == h, column, spread)
                gate_rep[d, s, g, :L] = spread

                for slot in range(SLOTS):
                    theirs = functools.reduce(jnp.logical_or, [helps(j, c) for j in slots if loans[j][3] == slot], z < 0)

                    @pl.when(jnp.logical_not(theirs))
                    def _(d=d, s=s, g=g, slot=slot):
                        gate_rep[d, s, g, L + slot * E : L + (slot + 1) * E] = jnp.full((E, C), -masked_score, f32)

    for s in range(S):
        fresh = jnp.dot(new_v[1, s : s + 1, :], qblock[s, 0], preferred_element_type=f32) * scale
        own_gate = jnp.sum(jnp.where(heads_eye, ng_v[s : s + 1, :], 0.0), axis=1, keepdims=True)
        fresh = jnp.where(last_block, fresh - as_row(gates_v[0, s, :, BL - 1 : BL] + own_gate), masked_score)
        weight = jnp.where(last_block, jnp.ones_like(fresh), 0.0)
        stats_tx[0, 0, s : s + 1, :] = fresh
        stats_tx[0, 1, s : s + 1, :] = weight
        stats_tx[0, 2, s : s + 1, :] = weight * new_v[2, s : s + 1, :].astype(f32)
        stats_tx[1, 0, s : s + 1, :] = jnp.full((1, C), masked_score, f32)
        stats_tx[1, 1, s : s + 1, :] = jnp.zeros((1, C), f32)
        stats_tx[1, 2, s : s + 1, :] = jnp.zeros((1, C), f32)

    pl.when(pauses)(lambda: by_block(lambda count: send(range(LEAD, HALF), count)))
    for d in range(1, X):
        for g in range(CORES):
            for j in slots:
                pl.when(lends(j, c))(gate_copy(d, g, j).start)
    for d in range(1, X):
        inv_copy(d).wait_recv()
        r = jnp.sum(jnp.where(eye, inv_rx[d - 1], 0.0), axis=1, keepdims=True)
        for k in range(RAW):
            x_arrival(d, k).wait_recv()
            rx[d - 1, k, :rows_each] = norm(rx[d - 1, k, :rows_each], r, k)

    def w_part(k):
        return wbuf[pl.ds(k * KC if isinstance(k, int) else pl.multiple_of(k * KC, KC), KC), :]

    def y_copy(d, s, v):
        at = pl.ds(pl.multiple_of(source(d) * L, L), L)
        return pltpu.make_async_remote_copy(
            ybuf.at[d, v, pl.ds(s * L, L)], (kbuf, vbuf)[v].at[s, at],
            sy_sem, ry_sem, device_id={"tp": partner}, device_id_type=MESH,
        )

    def rows_of(d, s):
        return L + EE if d and s == S - 1 else L

    def finish(d, y, first, prompts, last):
        pairs = [(g, s) for g in range(CORES) for s in prompts]
        before = {(g, s): [stats_tx[g, i, s : s + 1, :] for i in range(3)] for g, s in pairs}
        scores = {}
        for g, s in pairs:
            count = rows_of(d, s)
            keys = y[s * L - first : s * L - first + count, g * C : (g + 1) * C]
            scores[g, s] = jnp.dot(keys, qblock[s, g], preferred_element_type=f32) * scale - gate_rep[d, s, g, :count]
        after = {}
        for g, s in pairs:
            old_top, old_total, old_weighted = before[g, s]
            values = y[s * L - first : s * L - first + rows_of(d, s), (2 + g) * C : (3 + g) * C].astype(f32)
            top = jnp.maximum(jnp.max(scores[g, s], axis=0, keepdims=True), old_top)
            weights = jnp.exp(scores[g, s] - top)
            factor = jnp.exp(old_top - top)
            total = jnp.sum(weights, axis=0, keepdims=True) + factor * old_total
            weighted = jnp.sum(weights * values, axis=0, keepdims=True) + factor * old_weighted
            after[g, s] = (top, total, weighted)
        for g, s in pairs:
            for i, row in enumerate(after[g, s]):
                stats_tx[g, i, s : s + 1, :] = row
        if last:
            for s in prompts:
                for i, row in enumerate(after[0, s]):
                    stats_rx[0, z, i, s : s + 1, :] = row

    def deliver(d, y, first, prompts):
        place = pl.ds(pl.multiple_of(source(d) * L, L), L)
        for s in prompts:
            part = y[s * L - first : (s + 1) * L - first]
            kbuf[s, place, :] = part[:, :C]
            vbuf[s, place, :] = part[:, 2 * C : 3 * C]
            ybuf[d, 0, s * L : (s + 1) * L] = part[:, C : 2 * C]
            ybuf[d, 1, s * L : (s + 1) * L] = part[:, 3 * C :]

    def send_partner(d, prompts):
        for s in prompts:
            for v in range(2):
                y_copy(d, s, v).start()

    pltpu.make_async_copy(wbuf.at[:, pl.ds(0, 2 * C)], wbuf.at[:, pl.ds(0, 2 * C)], w_sem).wait()
    both_weights.wait_recv()

    for j in slots:

        @pl.when(helps(j, c))
        def _(j=j):
            lend(j).wait_recv()
            for d in range(1, X):
                forward(d, j).start()

    by_block(lambda count: send(range(HALF, split), count))
    for part in range(2):
        for k in range(split, NC):
            for d in range(1, X):
                by_block(lambda count: x_part(d, k, part, count).start())
    acc[...] = jnp.zeros_like(acc)

    def near(k, carry):
        acc[:rows_each] += jnp.dot(nb[k], w_part(k), preferred_element_type=f32)
        return carry

    lax.fori_loop(0, NC, near, 0)
    y = acc[:rows_each].astype(bf)
    deliver(0, y, 0, range(S))
    finish(0, y, 0, range(S), X == 1)
    send_partner(0, range(S))
    pl.semaphore_signal(ready_sem, inc=1, device_id={"tp": partner}, device_id_type=MESH)
    for d in range(1, X):
        for g in range(CORES):

            for j in slots:

                @pl.when(lends(j, c))
                def _(d=d, g=g, j=j):
                    gate_copy(d, g, j).wait_send()
                    back = L - loans[j][4]
                    gate_rep[d, S - 1, g, back : back + E] = jnp.full((E, C), -masked_score, f32)

                pl.when(helps(j, c))(gate_copy(d, g, j).wait_recv)
    pl.semaphore_wait(ready_sem, 1)

    for d in range(1, X):
        acc[...] = jnp.zeros_like(acc)

        def far(k, carry, d=d):
            acc[...] += jnp.dot(rx[d - 1, k], w_part(k), preferred_element_type=f32)
            return carry

        def far_arriving(k, carry, d=d):
            by_block(lambda count: x_arrival(d, k, count).wait_recv())
            return far(k, carry, d)

        for j in slots:
            pl.when(helps(j, c))(forward(d, j).wait_recv)
        lax.fori_loop(0, RAW, far, 0)
        lax.fori_loop(RAW, split, far_arriving, 0)
        last = d == X - 1
        if cut:
            for k in range(split, NC):
                x_part(d, k, 0).wait_recv()
                acc[:cut] += jnp.dot(rx[d - 1, k, :cut], w_part(k), preferred_element_type=f32)
            y = acc[:cut].astype(bf)
            finish(d, y, 0, range(S - 1), last)
            fronts = y
        for k in range(split, NC - 1):
            by_block(lambda count: x_part(d, k, 1, count).wait_recv())
            acc[cut:] += jnp.dot(rx[d - 1, k, cut:], w_part(k), preferred_element_type=f32)
        by_block(lambda count: x_part(d, NC - 1, 1, count).wait_recv())
        y = (acc[cut:] + jnp.dot(rx[d - 1, NC - 1, cut:], w_part(NC - 1), preferred_element_type=f32)).astype(bf)

        for j in slots:

            @pl.when(helps(j, c))
            def _(d=d, y=y, j=j):
                for g in range(CORES):
                    for v in range(2):
                        slot = loans[j][3]
                        rows_back = y[L + slot * E : L + (slot + 1) * E]
                        lent_tx[d - 1, g, slot, v] = rows_back[:, (2 * v + g) * C : (2 * v + g + 1) * C]
                    give_back(d, g, j).start()

        finish(d, y, cut, [S - 1], last)
        if not last:
            if cut:
                deliver(d, fronts, 0, range(S - 1))
            deliver(d, y, cut, [S - 1])
            send_partner(d, range(S))

    def z_target(i):
        return jnp.where(2 * z >= Z, i, Z - 1 - i)

    def z_copy(i, other):
        to = z_target(i)
        return pltpu.make_async_remote_copy(
            stats_tx.at[other], stats_rx.at[other, z], sz_sem.at[other], rz_sem.at[other],
            device_id={"sp": to, "tp": partner if other else tp}, device_id_type=MESH,
        )

    for i in range(Z):
        for first_core in range(CORES):

            @pl.when(c == first_core)
            def _(i=i, first_core=first_core):
                for core in range(CORES):
                    if core == first_core:
                        pl.when(z_target(i) != z)(z_copy(i, 0).start)
                    else:
                        z_copy(i, 1).start()

    if X > 1:
        if cut:
            deliver(X - 1, fronts, 0, range(S - 1))
        deliver(X - 1, y, cut, [S - 1])
        send_partner(X - 1, range(S))
    for d in range(1, X):
        inv_copy(d).wait_send()
        pl.when(jnp.logical_not(pauses))(x_sent(d, 0, RAW, 0).wait_send)
        pl.when(jnp.logical_not(pauses))(lambda: by_block(lambda count: x_sent(d, RAW, LEAD, 1, count).wait_send()))
        by_block(lambda count: x_sent(d, LEAD, NC, 2, count).wait_send())

        for j in slots:

            @pl.when(helps(j, c))
            def _(d=d, j=j):
                forward(d, j).wait_send()
                for g in range(CORES):
                    give_back(d, g, j).wait_send()

    for j in slots:
        pl.when(lends(j, c))(lend(j).wait_send)
    both_weights.wait_send()
    shares[2].wait_send()
    shares[3].wait_send()
    halves = pltpu.make_async_remote_copy(ybuf, ybuf, sy_sem, ry_sem, device_id={"tp": partner}, device_id_type=MESH)
    halves.wait_send()
    halves.wait_recv()

    def z_whole(other):
        part = stats_rx.at[other, pl.ds(0, Z - 1 + other)]
        return pltpu.make_async_remote_copy(
            part, part, sz_sem.at[other], rz_sem.at[other],
            device_id={"tp": partner if other else tp}, device_id_type=MESH,
        )

    for other in range(CORES):
        if Z - 1 + other:
            z_whole(other).wait_recv()

    for j in slots:
        for g in range(CORES):
            core = CORES - 1 - c if g else c

            @pl.when(lends(j, core))
            def _(g=g, j=j, core=core):
                for d in range(1, X):
                    give_back(d, g, j).wait_recv()
                    at = pl.ds(pl.multiple_of(((x + X - d) % X * CORES + core) * L + L - loans[j][4], E), E)
                    kbuf[S - 1, at, :] = lent_rx[d - 1, g, j, 0]
                    vbuf[S - 1, at, :] = lent_rx[d - 1, g, j, 1]

    entries = [(i, other) for i in range(Z) for other in range(CORES)]
    tops = [stats_rx[other, i, 0] for i, other in entries]
    most = functools.reduce(jnp.maximum, tops)
    factors = [jnp.exp(top - most) for top in tops]
    total = functools.reduce(jnp.add, [f * stats_rx[other, i, 1] for f, (i, other) in zip(factors, entries)])
    weighted = functools.reduce(jnp.add, [f * stats_rx[other, i, 2] for f, (i, other) in zip(factors, entries)])
    ro_ref[...] = (weighted / total).astype(ro_ref.dtype)
    for other in range(CORES):
        if Z - 1 + other:
            z_whole(other).wait_send()


def scoped(dims, semaphores, *refs):
    pl.run_scoped(lambda *held: kernel(dims, *refs, *held), *semaphores)


def write_out(*refs):
    count = len(refs) // 2

    def move(sems):
        copies = [pltpu.make_async_copy(refs[i], refs[count + i], sems.at[i]) for i in range(count)]
        for copy in copies:
            copy.start()
        for copy in copies:
            copy.wait()

    pl.run_scoped(move, pltpu.SemaphoreType.DMA((count,)))


def body(
    tokens, norm_gain, key_weight, value_weight, cum_gates, new_query, new_key, new_value, new_gate
):
    S, L, D = tokens.shape
    C = key_weight.shape[1]
    H = C // HD
    T = lax.axis_size("tp")
    Z = lax.axis_size("sp")
    X = T // CORES
    BL = T * L
    R = 32 if L % 32 == 0 else L
    KC = 256 if D % 256 == 0 else D // 2
    NC = D // KC
    bf, f32 = jnp.bfloat16, jnp.float32
    hbm = pl.BlockSpec(memory_space=pltpu.HBM)
    dma = pltpu.SemaphoreType.DMA
    regular = pltpu.SemaphoreType.REGULAR
    far = max(X - 1, 1)
    vmem = pl.BlockSpec(memory_space=pltpu.VMEM)
    semaphores = [
        dma((S * L // R,)), dma((RAW,)), dma, dma((4,)), regular((max(Z - 2, 1),)), regular, regular,
        dma((far, 3)), dma((far, NC + TAIL)), dma((far,)), dma((far,)), dma((3,)), dma((3,)),
        dma, dma, dma((CORES,)), dma((CORES,)),
        dma((3,)), dma((3,)), dma((far, 3)), dma((far, 3)),
        *(dma((far, CORES, 3)) for _ in range(4)),
    ]
    results = pl.pallas_call(
        functools.partial(scoped, (S, L, R, T, Z), semaphores),
        out_shape=(
            pltpu.VMEM((S, BL, C), bf),
            pltpu.VMEM((S, BL, C), bf),
            pltpu.VMEM((S, C), bf),
        ),
        in_specs=[hbm] * 9,
        out_specs=(vmem, vmem, vmem),
        scratch_shapes=[
            pltpu.VMEM((S * L, D), bf),
            pltpu.VMEM((RAW, S * L, KC), bf),
            pltpu.VMEM((S * L, KC), f32),
            pltpu.VMEM((NC, S * L, KC), bf),
            pltpu.VMEM((far, NC, S * L + SLOTS * EXTRA, KC), bf),
            pltpu.VMEM((S * L + SLOTS * EXTRA, 4 * C), f32),
            pltpu.VMEM((D, 4 * C), bf),
            pltpu.VMEM((X, 2, S * L, C), bf),
            pltpu.VMEM((D // 128, 128), bf),
            pltpu.VMEM((1, D), f32),
            pltpu.VMEM((CORES, S, H, BL), f32),
            pltpu.VMEM((4, S, C), bf),
            pltpu.VMEM((S, H), f32),
            pltpu.VMEM((1, S * L), f32),
            pltpu.VMEM((far, 1, S * L), f32),
            pltpu.VMEM((S, CORES, C, C), bf),
            pltpu.VMEM((X, S, CORES, L + SLOTS * EXTRA, C), f32),
            pltpu.VMEM((CORES, 3, S, C), f32),
            pltpu.VMEM((CORES, Z, 3, S, C), f32),
            pltpu.VMEM((SLOTS, NC, EXTRA, KC), bf),
            pltpu.VMEM((far, CORES, SLOTS, 2, EXTRA, C), bf),
            pltpu.VMEM((far, CORES, 3, 2, EXTRA, C), bf),
        ],
        compiler_params=pltpu.CompilerParams(
            collective_id=0, has_side_effects=True, vmem_limit_bytes=56 * 1024 * 1024
        ),
    )(
        tokens.reshape(S * L, D),
        norm_gain.reshape(D // 128, 128),
        key_weight,
        value_weight,
        jnp.transpose(cum_gates, (0, 2, 1)),
        new_query,
        new_key,
        new_value,
        new_gate,
    )
    return pl.pallas_call(
        write_out,
        out_shape=tuple(jax.ShapeDtypeStruct(r.shape, r.dtype) for r in results),
        in_specs=[vmem] * 3,
        out_specs=(hbm, hbm, hbm),
    )(*(pltpu.with_memory_space_constraint(r, pltpu.VMEM) for r in results))


def solution(mesh):
    in_specs = (
        P("gr", ("sp", "tp"), None),
        P(),
        P(None, "tp"),
        P(None, "tp"),
        P("gr", "sp", "tp"),
        P("gr", "tp"),
        P("gr", "tp"),
        P("gr", "tp"),
        P("gr", "tp"),
    )
    out_specs = (P("gr", "sp", "tp"), P("gr", "sp", "tp"), P("gr", "tp"))
    return jax.shard_map(body, mesh=mesh, in_specs=in_specs, out_specs=out_specs, check_vma=False)
```
